512 devices in a mesh: grp: 2 (over y), ep: 32 (over z, core), tp: 8 (over x).
Axes of the slice: x: 8, y: 2, z: 16, core: 2. Of those that a mesh axis runs over, the one named last changes fastest.
The devices are a block of a 8x8x16 slice.
Arguments:
- scan_branch_source: bfloat16 [8192, 1344], P(('grp', 'ep'), 'tp'), parts along dimension 0, may hold values from -8 to 8
- valve_branch_source: bfloat16 [8192, 1344], P(('grp', 'ep'), 'tp'), parts along dimension 0, may hold values from -6 to 6
- stencil_factors: bfloat16 [4, 1344], P(None, 'tp'), may hold values from -3 to 3
- carry_valve_matrix: bfloat16 [8, 168, 168], P('tp'), may hold values from -0.5 to 0.5
- entry_valve_matrix: bfloat16 [8, 168, 168], P('tp'), may hold values from -0.5 to 0.5
- lane_fade_param: float32 [1344], P('tp'), may hold values from 0 to 16
- jump_log_fade: float32 [8192], P(('grp', 'ep')), parts along dimension 0, may hold values from -0.6 to 0, as said below
- specialist_entries: bfloat16 [16384, 2048], P(('grp', 'ep')), parts along dimension 0, may hold values from -6 to 6
- specialist_rms_scale: float32 [2048], replicated, may hold values from 0.1 to 1.9
- assigned_specialists: int32 [16384, 2], P(('grp', 'ep')), parts along dimension 0, may hold values from 0 to 31, all different within a row; in each aligned block of 256 rows (0 to 255, 256 to 511, ...) at most 24 rows name the same one
- picked_route_scores: float32 [16384, 2], P(('grp', 'ep')), parts along dimension 0, may hold values from -6 to 6
- expand_matrix: bfloat16 [32, 2048, 3584], P('ep', None, 'tp'), may hold values from -0.125 to 0.125
- contract_matrix: bfloat16 [32, 3584, 2048], P('ep', None, 'tp'), may hold values from -0.09375 to 0.09375
Outputs:
- valved_scan_target: bfloat16 [8192, 1344], P(('grp', 'ep'), 'tp'), parts along dimension 0
- moe_out: bfloat16 [16384, 2048], P(('grp', 'ep'), 'tp'), parts along dimension 0
The draws below stay inside these ranges and needn't reach their ends.
There are 2 independent parts, one for each index of `grp`. The reference program is written for one: setup_inputs(seed, part) draws one part's arguments, and reference() takes and returns one part's arrays. A program takes and returns all parts, laid end to end along the dimension named above; an argument that names none is the same for every part. Nothing has to cross between parts.
Inputs may be any that keep to these rules, and one draw needn't show every extreme that they name: `assigned_specialists`: each row names 2 different experts. Among the tokens of one index of ep (aligned blocks of 256 rows) no expert is named more than 24 times, and in some block some expert is named exactly 24 times. `jump_log_fade`: zero at all but a few positions.
All inputs are finite; a program needn't handle non-finite values.
Results may differ from the reference program's by a relative error of at most 0.0065.
Values may be sent and summed in bfloat16 or wider, within the bound.
No kernel may reach another device: no remote copies, remote signals or barrier semaphores. Data moves between devices by JAX's collectives and lax.ppermute only.
A program may use at most 128 MiB of HBM per device.

```python
import math
from functools import partial
import jax
import jax.numpy as jnp
import numpy as np
from jax import lax

D = 2048
FF = 3584
BW = 168
BLOCKS = 8
CONV = 4
TOPK = 2
MX_DEV = 128
MT_DEV = 256
CH = 1344
EXPERTS = 32
SEQUENCE_POINTS = 4096
MTOK = 8192
CAP = 24
N_EP = 32


def draw_scan_branch_source(key, part):
    scale_key, base_key = jax.random.split(jax.random.fold_in(key, 11))
    block_count = SEQUENCE_POINTS // MX_DEV
    scales = jnp.exp(jax.random.uniform(scale_key, (block_count,), jnp.float32, jnp.log(0.5), jnp.log(2.0)))
    row_scale = scales[jnp.arange(SEQUENCE_POINTS) // MX_DEV]
    base_draw = jnp.clip(jax.random.normal(base_key, (SEQUENCE_POINTS, CH), jnp.float32), -4.0, 4.0)
    return (base_draw * row_scale[:, None]).astype(jnp.bfloat16)


def draw_lane_fade_param(key, part):
    pick_key, fast_key, slow_key = jax.random.split(jax.random.fold_in(key, 23), 3)
    fast_share = 0.5
    fast_pick = jax.random.bernoulli(pick_key, fast_share, (CH,))
    fast_rate = jnp.exp(jax.random.uniform(fast_key, (CH,), jnp.float32, jnp.log(1.0 / MX_DEV), jnp.log(3.0 / MX_DEV)))
    slow_rate = jnp.exp(jax.random.uniform(slow_key, (CH,), jnp.float32, jnp.log(0.01 / SEQUENCE_POINTS), jnp.log(0.1 / SEQUENCE_POINTS)))
    decay_rate = jnp.where(fast_pick, fast_rate, slow_rate)
    return (-jnp.log(jnp.expm1(decay_rate))).astype(jnp.float32)


def draw_jump_log_fade(key, part):
    location_random_key, height_random_key = jax.random.split(jax.random.fold_in(key, 37))
    spike_locations = jax.random.randint(location_random_key, (3,), 0, SEQUENCE_POINTS)
    spike_height = jax.random.uniform(height_random_key, (3,), jnp.float32, jnp.log(0.55), jnp.log(0.8))
    return jnp.zeros((SEQUENCE_POINTS,), jnp.float32).at[spike_locations].set(spike_height)


def levels(own_key, extent, cuts, least, top_value):
    loudness, own = 1.0, jax.random.fold_in(own_key, 6)
    for dim, parts in cuts:
        steps = jnp.exp(jax.random.uniform(jax.random.fold_in(own, dim), (parts,), jnp.float32, least / len(cuts), top_value / len(cuts)))
        loudness = loudness * jnp.repeat(steps, extent[dim] // parts).reshape([-1 if axis == dim else 1 for axis in range(len(extent))])
    return loudness


def shared_out(own_key, own, number, rows, count, top, reach, skew):
    sequence = jax.random.permutation(own_key, count)
    crowded, common = portions_of(count, rows * top, reach, skew, True), portions_of(count, rows * top, reach, skew, False)
    places = jnp.arange(count)

    def named(tallies, offset_by):
        used = int((tallies > 0).sum())
        fixed = max(1, used // 4)
        shifted = fixed + (places - fixed + offset_by * (used - fixed)) % max(1, count - fixed)
        return jnp.zeros((count,), jnp.int32).at[sequence[jnp.where(places < fixed, places, shifted)]].set(jnp.asarray(tallies, jnp.int32))

    tallies = jnp.where(number % 4 == 0, named(crowded, number // 4), named(common, number - number // 4 - 1))
    mixed = jax.random.permutation(jax.random.fold_in(own, 3), count)
    donor, receiver = mixed[0:count // 2 * 2:2], mixed[1:count // 2 * 2:2]
    margin = jnp.minimum(tallies[donor] - 1, reach - tallies[receiver]) // 2
    margin = jnp.where((donor == sequence[0]) | (receiver == sequence[0]) | (tallies[receiver] == 0), 0, jnp.maximum(margin, 0))
    shifted = jax.random.randint(jax.random.fold_in(own, 4), (count // 2,), 0, 1 << 20) % (margin + 1)
    tallies = tallies.at[donor].add(-shifted).at[receiver].add(shifted)
    members = jnp.searchsorted(jnp.cumsum(tallies), jnp.arange(rows * top), side="right").astype(jnp.int32)
    listing = members.reshape(top, rows).T
    listing = listing[jax.random.permutation(jax.random.fold_in(own, 1), rows)]
    offset_by = jax.random.randint(jax.random.fold_in(own, 2), (rows, 1), 0, top)
    return jnp.take_along_axis(listing, (jnp.arange(top)[None, :] + offset_by) % top, axis=1)


def portions_of(count, total, bound, lean, full):
    loads = [(1 << 20) // math.isqrt(grade ** lean) + 1 for grade in range(1, count + 1)]
    largest = bound if full else min(bound, max(-(-total // count), total * loads[0] // sum(loads)))
    least = 1 if total - largest >= count - 1 else 0
    counts, rest = [largest] + [least] * (count - 1), total - largest - least * (count - 1)
    while rest > 0:
        movable = [i for i in range(1, count) if counts[i] < largest] or [i for i in range(1, count) if counts[i] < bound]
        whole, budget = sum([loads[i] for i in movable]), rest
        for i in movable:
            addition = min(bound - counts[i], max(1, budget * loads[i] // whole), rest)
            counts[i] = counts[i] + addition
            rest = rest - addition
    return np.array(counts)


def scatter_about(key, dims, deviation, bound, pieces=(), kind=jnp.bfloat16):
    result = jax.random.normal(key, dims, jnp.float32) * deviation
    if len(pieces) > 0:
        result = levels(key, dims, pieces, -0.22, 0.18) * result
    return jnp.clip(result, min=-bound, max=bound).astype(kind)


def setup_inputs(seed: int = 0, part: int = 0) -> dict:
    key_of = jax.random.split(jax.random.key(seed), 14)
    own_keys = jax.random.split(jax.random.fold_in(key_of[13], part), 14)
    scan_branch_source = draw_scan_branch_source(jax.random.fold_in(jax.random.fold_in(key_of[13], part), 71), part)
    valve_branch_source = scatter_about(own_keys[1], (SEQUENCE_POINTS, CH), 1.0, 6.0, ((0, 32), (1, 8)))
    stencil_factors = scatter_about(key_of[2], (CONV, CH), CONV ** -0.5, 3.0, ((1, 8),))
    carry_valve_matrix = scatter_about(key_of[3], (BLOCKS, BW, BW), BW ** -0.5, 0.5, ((0, 8),))
    entry_valve_matrix = scatter_about(key_of[4], (BLOCKS, BW, BW), BW ** -0.5, 0.5, ((0, 8),))
    lane_fade_param = draw_lane_fade_param(jax.random.fold_in(key_of[13], 71), part)
    jump_log_fade = draw_jump_log_fade(jax.random.fold_in(jax.random.fold_in(key_of[13], part), 71), part)
    specialist_entries = scatter_about(own_keys[7], (MTOK, D), 1.0, 6.0, ((0, 32),))
    specialist_rms_scale = jnp.clip(1.0 + 0.18 * jax.random.normal(key_of[8], (D,), jnp.float32), 0.1, 1.9)
    assigned_specialists_keys = jax.random.split(jax.random.fold_in(own_keys[9], 1), MTOK // MT_DEV)
    assigned_specialists_turns = jax.random.permutation(jax.random.fold_in(own_keys[9], 3), MTOK // MT_DEV)
    assigned_specialists = jax.vmap(lambda own, number: shared_out(jax.random.fold_in(own_keys[9], 2), own, number, MT_DEV, EXPERTS, TOPK, CAP, 1))(assigned_specialists_keys, assigned_specialists_turns).reshape((MTOK, TOPK))
    picked_route_scores = scatter_about(own_keys[10], (MTOK, TOPK), 1.5, 6.0, ((0, 32),), jnp.float32)
    expand_matrix = scatter_about(key_of[11], (EXPERTS, D, FF), D ** -0.5, 0.125, ((0, 32), (2, 8)))
    contract_matrix = scatter_about(key_of[12], (EXPERTS, FF, D), FF ** -0.5, 0.09375, ((0, 32), (2, 8)))
    return dict(scan_branch_source=scan_branch_source, valve_branch_source=valve_branch_source, stencil_factors=stencil_factors, carry_valve_matrix=carry_valve_matrix, entry_valve_matrix=entry_valve_matrix, lane_fade_param=lane_fade_param, jump_log_fade=jump_log_fade, specialist_entries=specialist_entries, specialist_rms_scale=specialist_rms_scale, assigned_specialists=assigned_specialists, picked_route_scores=picked_route_scores, expand_matrix=expand_matrix, contract_matrix=contract_matrix)


def chain_link(earlier, later):
    early_decay, early_state = earlier
    late_decay, late_state = later
    return (early_decay * late_decay, late_decay * early_state + late_state)

def slot_table(assigned_specialists, experts, capacity):
    flat_routes = assigned_specialists.reshape(-1)
    top_count = assigned_specialists.shape[1]
    matches = (flat_routes[:, None] == jnp.arange(experts, dtype=jnp.int32)[None, :]).astype(jnp.int32)
    before = jnp.cumsum(matches, axis=0) - matches
    slot_rank = lax.optimization_barrier(jnp.sum(before * matches, axis=1))
    slot_index = (flat_routes * capacity + slot_rank).astype(jnp.int32)
    owner_row = (jnp.arange(flat_routes.shape[0], dtype=jnp.int32) // top_count).astype(jnp.int32)
    source = jnp.zeros((experts * capacity,), jnp.int32).at[slot_index].set(owner_row)
    filled = jnp.zeros((experts * capacity,), jnp.float32).at[slot_index].set(1.0)
    return (slot_index, source, filled)

def temporal_block_part(scan_branch_source, valve_branch_source, stencil_factors, carry_valve_matrix, entry_valve_matrix, lane_fade_param, jump_log_fade):
    length = scan_branch_source.shape[0]
    channels = scan_branch_source.shape[1]
    padded = jnp.pad(scan_branch_source.astype(jnp.float32), ((CONV - 1, 0), (0, 0)))
    tap_values = stencil_factors.astype(jnp.float32)
    conv_out = jnp.zeros((length, channels), jnp.float32)
    for offset in range(CONV):
        conv_out = conv_out + padded[offset:offset + length] * tap_values[offset]
    conv_half = lax.optimization_barrier(conv_out.astype(jnp.bfloat16))
    conv_blocks = conv_half.astype(jnp.float32).reshape(length, BLOCKS, BW)
    carry_valve = jax.nn.sigmoid(jnp.einsum('tnc,ncd->tnd', conv_blocks, carry_valve_matrix.astype(jnp.float32), precision=lax.Precision.HIGHEST).reshape(length, channels))
    input_gate = jax.nn.sigmoid(jnp.einsum('tnc,ncd->tnd', conv_blocks, entry_valve_matrix.astype(jnp.float32), precision=lax.Precision.HIGHEST).reshape(length, channels))
    fade_log_rate = -8.0 * carry_valve * jax.nn.softplus(-lane_fade_param)[None, :] + jump_log_fade[:, None]
    drive_term = jnp.sqrt(-jnp.expm1(2.0 * fade_log_rate)) * input_gate * conv_out
    cumulative, hidden_state = lax.associative_scan(chain_link, (jnp.exp(fade_log_rate), drive_term), axis=0)
    return (hidden_state * jax.nn.gelu(valve_branch_source.astype(jnp.float32))).astype(jnp.bfloat16)

def expert_part(specialist_entries, specialist_rms_scale, assigned_specialists, picked_route_scores, expand_matrix, contract_matrix):
    tok_rows = specialist_entries.astype(jnp.float32)
    row_mean = lax.optimization_barrier(jnp.mean(tok_rows, axis=1, keepdims=True))
    centered = tok_rows - row_mean
    row_var = lax.optimization_barrier(jnp.mean(centered * centered, axis=1, keepdims=True))
    normed = (centered * lax.rsqrt(row_var + 1e-05) * specialist_rms_scale[None, :]).astype(jnp.bfloat16)
    blocks = assigned_specialists.reshape(N_EP, MT_DEV, TOPK)
    slots, sources, filled = jax.vmap(partial(slot_table, experts=EXPERTS, capacity=CAP))(blocks)
    offsets = (jnp.arange(N_EP, dtype=jnp.int32) * MT_DEV)[:, None]
    global_source = (sources + offsets).reshape(N_EP, EXPERTS, CAP).transpose(1, 0, 2)
    global_filled = filled.reshape(N_EP, EXPERTS, CAP).transpose(1, 0, 2)

    def one_expert(inputs):
        source, mask_rows, up_part, down_part = inputs
        picked = normed[source.reshape(-1)] * mask_rows.reshape(-1, 1).astype(jnp.bfloat16)
        hidden = jax.nn.silu(jnp.dot(picked, up_part, preferred_element_type=jnp.float32)).astype(jnp.bfloat16)
        return jnp.dot(hidden, down_part, preferred_element_type=jnp.float32).astype(jnp.bfloat16)
    results = lax.map(one_expert, (global_source, global_filled, expand_matrix, contract_matrix))
    results = results.reshape(EXPERTS, N_EP, CAP, D)
    slot_index = slots.reshape(N_EP, MT_DEV * TOPK)
    expert_index = slot_index // CAP
    rank_index = slot_index % CAP
    block_index = jnp.broadcast_to(jnp.arange(N_EP, dtype=jnp.int32)[:, None], slot_index.shape)
    picked = results[expert_index, block_index, rank_index].reshape(MTOK, TOPK, D).astype(jnp.float32)
    first_weight = jax.nn.sigmoid(picked_route_scores[:, 0] - picked_route_scores[:, 1])
    weights = jnp.stack([first_weight, 1.0 - first_weight], axis=1)
    return lax.optimization_barrier(jnp.sum(weights[:, :, None] * picked, axis=1)).astype(jnp.bfloat16)

def reference(scan_branch_source, valve_branch_source, stencil_factors, carry_valve_matrix, entry_valve_matrix, lane_fade_param, jump_log_fade, specialist_entries, specialist_rms_scale, assigned_specialists, picked_route_scores, expand_matrix, contract_matrix):
    valved_scan_target = temporal_block_part(scan_branch_source, valve_branch_source, stencil_factors, carry_valve_matrix, entry_valve_matrix, lane_fade_param, jump_log_fade)
    moe_out = expert_part(specialist_entries, specialist_rms_scale, assigned_specialists, picked_route_scores, expand_matrix, contract_matrix)
    return (valved_scan_target, moe_out)
```

```python
import functools

import jax
import jax.numpy as jnp
from jax import lax
from jax.experimental import pallas as pl
from jax.experimental.pallas import tpu as pltpu
from jax.sharding import PartitionSpec as P

CONV = 4
CAPACITY = 24
F32 = jnp.float32
BF16 = jnp.bfloat16

NN = (((1,), (0,)), ((), ()))
NT = (((1,), (1,)), ((), ()))


def dot(a, b, dims=NN):
    return lax.dot_general(a, b, dims, preferred_element_type=F32)


def vmem():
    return pl.BlockSpec(memory_space=pltpu.VMEM)


def cost(flops, nbytes):
    return pl.CostEstimate(flops=flops, bytes_accessed=nbytes, transcendentals=0)


def grant(mebibytes):
    return pltpu.CompilerParams(vmem_limit_bytes=mebibytes * 2**20)


def one_hots(routes, experts):
    lanes = lax.broadcasted_iota(jnp.int32, (routes.shape[0], experts), 1)
    return [(routes[:, k : k + 1] == lanes).astype(F32) for k in range(2)]


def dispatch_kernel(at_ref, tok_ref, scale_ref, routes_ref, out_ref):
    tokens, features = tok_ref.shape
    slots, width = out_ref.shape
    experts = slots // CAPACITY
    first = pl.multiple_of(at_ref[0], width)
    rows = tok_ref[...].astype(F32)
    mean = jnp.sum(rows, axis=1, keepdims=True) * (1.0 / features)
    centered = rows - mean
    var = jnp.sum(centered * centered, axis=1, keepdims=True) * (1.0 / features)
    part = tok_ref[:, pl.ds(first, width)].astype(F32) - mean
    normed = (part * lax.rsqrt(var + 1e-05) * scale_ref[:, pl.ds(first, width)]).astype(BF16)
    hot = [m.astype(BF16) for m in one_hots(routes_ref[...], experts)]
    eye = (
        lax.broadcasted_iota(jnp.int32, (experts, experts), 0)
        == lax.broadcasted_iota(jnp.int32, (experts, experts), 1)
    ).astype(F32).astype(BF16)
    named = [dot(eye, m, NT) for m in hot]
    earlier = (
        lax.broadcasted_iota(jnp.int32, (tokens, tokens), 0)
        < lax.broadcasted_iota(jnp.int32, (tokens, tokens), 1)
    ).astype(F32).astype(BF16)
    base = lax.broadcasted_iota(jnp.int32, (experts, tokens), 0).astype(F32) * CAPACITY
    place = base + dot((named[0] + named[1]).astype(BF16), earlier)
    slot = [jnp.sum(m * place, axis=0, keepdims=True).astype(jnp.int32) for m in named]
    ids = lax.broadcasted_iota(jnp.int32, (slots, tokens), 0)
    pick = jnp.logical_or(ids == slot[0], ids == slot[1]).astype(F32).astype(BF16)
    out_ref[...] = dot(pick, normed).astype(BF16)


def dispatch(tok, scale, routes, at, experts, width):
    slots = experts * CAPACITY
    return pl.pallas_call(
        dispatch_kernel,
        out_shape=jax.ShapeDtypeStruct((slots, width), BF16),
        in_specs=[pl.BlockSpec(memory_space=pltpu.SMEM), vmem(), vmem(), vmem()],
        out_specs=vmem(),
        cost_estimate=cost(2 * slots * tok.shape[0] * width, 2 * tok.size + 2 * slots * width),
        compiler_params=grant(12),
        name="dispatch",
    )(at, tok, scale, routes)


def combine_kernel(ret_ref, routes_ref, score_ref, out_ref):
    slots = ret_ref.shape[0]
    tokens = routes_ref.shape[0]
    experts = slots // CAPACITY
    hot = one_hots(routes_ref[...], experts)
    earlier = (
        lax.broadcasted_iota(jnp.int32, (tokens, tokens), 1)
        < lax.broadcasted_iota(jnp.int32, (tokens, tokens), 0)
    ).astype(F32).astype(BF16)
    base = lax.broadcasted_iota(jnp.int32, (tokens, experts), 1).astype(F32) * CAPACITY
    place = base + dot(earlier, (hot[0] + hot[1]).astype(BF16))
    ids = lax.broadcasted_iota(jnp.int32, (tokens, slots), 1)
    picked = []
    for m in hot:
        slot = jnp.sum(m * place, axis=1, keepdims=True).astype(jnp.int32)
        picked.append(dot((ids == slot).astype(F32).astype(BF16), ret_ref[...]))
    weight = jax.nn.sigmoid(score_ref[:, 0:1] - score_ref[:, 1:2])
    out_ref[...] = (weight * picked[0] + (1.0 - weight) * picked[1]).astype(BF16)


def combine(returned, routes, scores):
    slots, width = returned.shape
    tokens = routes.shape[0]
    return pl.pallas_call(
        combine_kernel,
        out_shape=jax.ShapeDtypeStruct((tokens, width), BF16),
        in_specs=[vmem(), vmem(), vmem()],
        out_specs=vmem(),
        cost_estimate=cost(4 * slots * tokens * width, 2 * slots * width),
        compiler_params=grant(12),
        name="combine",
    )(returned, routes, scores)


def ring(block, axis):
    size = lax.axis_size(axis)
    ahead = [(i, (i + 1) % size) for i in range(size)]
    back = [(i, (i - 1) % size) for i in range(size)]
    left = right = block
    pieces = [block]
    for _ in range(size // 2 - 1):
        left = lax.ppermute(left, axis, ahead)
        right = lax.ppermute(right, axis, back)
        pieces += [left, right]
    far = (lax.ppermute(left[0], axis, ahead), lax.ppermute(right[1], axis, back))
    return pieces, far


def owners(axis):
    size = lax.axis_size(axis)
    steps = [0]
    for s in range(1, size // 2):
        steps += [-s, s]
    steps.append(size // 2)
    return ((lax.axis_index(axis) + jnp.array(steps)) % size).astype(jnp.int32)


def up_kernel(count, first, last, at_ref, *refs):
    pieces, refs = refs[:count], refs[count:]
    far, refs = (refs[:2], refs[2:]) if last else ((), refs)
    total_ref, refs = (None, refs) if first else (refs[0], refs[1:])
    w_ref, out_ref = refs
    width = pieces[0].shape[2]
    units = w_ref.shape[1]

    def rows(k):
        return w_ref[pl.ds(pl.multiple_of(at_ref[k] * width, width), width), :]

    for side in range(2):
        total = None if first else total_ref[side]
        for k, piece in enumerate(pieces):
            term = dot(piece[side], rows(k))
            total = term if total is None else total + term
        if last:
            total = total + dot(far[side][...], rows(count))
            hidden = total * jax.nn.sigmoid(total)
            out_ref[:, side * units : (side + 1) * units] = hidden.astype(BF16)
        else:
            out_ref[side] = total


def down_kernel(count, first, last, at_ref, *refs):
    pieces, refs = refs[:count], refs[count:]
    far, refs = (refs[:2], refs[2:]) if last else ((), refs)
    total_ref, refs = (None, refs) if first else (refs[0], refs[1:])
    w_ref, out_ref = refs
    rows, both = pieces[0].shape[1:]
    deep = w_ref.shape[1] - (w_ref.shape[1] - both // 2) // 2
    edge = w_ref.shape[1] - deep

    def term(block, k, side):
        if side == 0:
            return dot(block[:, 0:deep], w_ref[at_ref[k], edge : edge + deep])
        return dot(block[:, both - deep : both], w_ref[at_ref[k], 0:deep])

    for side in range(2):
        for part in range(2):
            span = slice(part * rows, (part + 1) * rows)
            total = None if first else total_ref[side, span]
            for k, piece in enumerate(pieces):
                value = term(piece.at[part], k, side)
                total = value if total is None else total + value
            if last:
                total = total + term(far[part], count, side)
            out_ref[side, span] = total.astype(out_ref.dtype)


def stage(body, name, pieces, far, total, at, w, out):
    operands = [*pieces, *far, *([] if total is None else [total]), w]
    kernel = functools.partial(body, len(pieces), total is None, len(far) > 0)
    share = len(pieces) + len(far) / 2
    macs = share * pieces[0].size * w.shape[-1]
    return pl.pallas_call(
        kernel,
        out_shape=out,
        in_specs=[pl.BlockSpec(memory_space=pltpu.SMEM)] + [vmem()] * len(operands),
        out_specs=vmem(),
        cost_estimate=cost(int(2 * macs), int(2 * share * pieces[0].size + 2 * w.size)),
        compiler_params=grant(20),
        name=name,
    )(at, *operands)


def staged(body, name, block, w, middle, out):
    pieces, far = ring(block, "tp")
    at = owners("tp")
    cut = len(pieces) - 2
    total = stage(body, name + "_near", pieces[:cut], (), None, at[:cut], w, middle)
    return stage(body, name + "_far", pieces[cut:], far, total, at[cut:], w, out)


def up(block, w):
    _, half, width = block.shape
    units = w.shape[1]
    middle = jax.ShapeDtypeStruct((2, half, units), F32)
    out = jax.ShapeDtypeStruct((half, 2 * units), BF16)
    return staged(up_kernel, "up", block, w, middle, out)


def down(block, w):
    _, rows, both = block.shape
    width = w.shape[1]
    units = both // 2
    edge = -units % 128
    padded = jnp.pad(w.reshape(-1, units, width), ((0, 0), (edge, edge), (0, 0)))
    middle = jax.ShapeDtypeStruct((2, 2 * rows, width), F32)
    out = jax.ShapeDtypeStruct((2, 2 * rows, width), BF16)
    return staged(down_kernel, "down", block, padded, middle, out)


def one_minus_exp(y):
    small = -y * (1.0 + y * (0.5 + y * (1.0 / 6 + y * (1.0 / 24 + y * (1.0 / 120 + y / 720)))))
    return jnp.where(y > -0.25, small, 1.0 - jnp.exp(y))


def local_kernel(x_ref, prev_ref, tap_ref, carry_ref, entry_ref, rate_ref, jump_ref, decay_ref, state_ref, ends_ref, pad_ref):
    length, channels = x_ref.shape
    pad_ref[0:8, :] = jnp.zeros((8, channels), F32)
    pad_ref[8 - (CONV - 1) : 8, :] = prev_ref[...].astype(F32)
    pad_ref[8 : 8 + length, :] = x_ref[...].astype(F32)
    taps = tap_ref[...].astype(F32)
    conv = jnp.zeros((length, channels), F32)
    for j in range(CONV):
        at = 8 - (CONV - 1) + j
        conv = conv + pad_ref[at : at + length, :] * taps[j : j + 1]
    half = conv.astype(BF16)
    recur = jax.nn.sigmoid(dot(half, carry_ref[0]))
    entry = jax.nn.sigmoid(dot(half, entry_ref[0]))
    log_decay = recur * rate_ref[...] + jump_ref[...]
    state = jnp.sqrt(one_minus_exp(2.0 * log_decay)) * entry * conv
    decay = jnp.exp(log_decay)
    rows = lax.broadcasted_iota(jnp.int32, (length, channels), 0)
    step = 1
    while step < length:
        ready = rows >= step
        before_state = jnp.where(ready, pltpu.roll(state, step, 0), 0.0)
        before_decay = jnp.where(ready, pltpu.roll(decay, step, 0), 1.0)
        state = decay * before_state + state
        decay = decay * before_decay
        step *= 2
    decay_ref[...] = decay
    state_ref[...] = state
    ends_ref[0:1, :] = decay[length - 1 : length]
    ends_ref[1:2, :] = state[length - 1 : length]


def local_scan(x, prev, taps, carry, entry, rate, jump):
    length, channels = x.shape
    full = jax.ShapeDtypeStruct((length, channels), F32)
    return pl.pallas_call(
        local_kernel,
        out_shape=(full, full, jax.ShapeDtypeStruct((2, channels), F32)),
        in_specs=[vmem()] * 7,
        out_specs=(vmem(), vmem(), vmem()),
        scratch_shapes=[pltpu.VMEM((length + 8, channels), F32)],
        cost_estimate=cost(100 * length * channels, 16 * length * channels),
        compiler_params=grant(6),
        name="local_scan",
    )(x, prev, taps, carry, entry, rate, jump)


def carry_kernel(at_ref, ends_ref, decay_ref, state_ref, valve_ref, out_ref):
    devices = ends_ref.shape[0]
    me = at_ref[0]
    entering = jnp.zeros((1, out_ref.shape[1]), F32)
    for d in range(devices):
        entering = jnp.where(
            d < me, ends_ref[d, 0:1, :] * entering + ends_ref[d, 1:2, :], entering
        )
    state = state_ref[...] + decay_ref[...] * entering
    valve = valve_ref[...].astype(F32)
    out_ref[...] = (state * jax.nn.gelu(valve, approximate=True)).astype(BF16)


def carry_in(ends, decay, state, valve, at):
    return pl.pallas_call(
        carry_kernel,
        out_shape=jax.ShapeDtypeStruct(valve.shape, BF16),
        in_specs=[pl.BlockSpec(memory_space=pltpu.SMEM)] + [vmem()] * 4,
        out_specs=vmem(),
        cost_estimate=cost(30 * valve.size, 12 * valve.size),
        compiler_params=grant(6),
        name="carry_in",
    )(at, ends, decay, state, valve)


def temporal(x, valve, taps, carry, entry, lane, jump):
    length = x.shape[0]
    size = lax.axis_size("ep")
    prev = lax.ppermute(x[length - (CONV - 1) :], "ep", [(i, i + 1) for i in range(size - 1)])
    rate = (-8.0 * jax.nn.softplus(-lane))[None, :]
    decay, state, ends = local_scan(x, prev, taps, carry, entry, rate, jump[:, None])
    spread = jnp.broadcast_to(ends[None], (size, *ends.shape))
    everyone = lax.all_to_all(spread, "ep", 0, 0, tiled=True)
    me = lax.axis_index("ep").astype(jnp.int32).reshape(1)
    return carry_in(everyone, decay, state, valve, me)


def expert(tok, scale, routes, scores, expand, contract):
    ep = lax.axis_size("ep")
    tp = lax.axis_size("tp")
    width = tok.shape[1] // tp
    at = (lax.axis_index("tp") * width).astype(jnp.int32).reshape(1)
    sent = dispatch(tok, scale[None, :], routes, at, ep, width)
    arrived = lax.all_to_all(sent.reshape(ep, CAPACITY, width), "ep", 0, 0, tiled=True)
    half = ep * CAPACITY // 2
    hidden = up(arrived.reshape(2, half, width), expand[0])
    done = down(hidden.reshape(2, half // 2, -1), contract[0])
    returned = lax.all_to_all(done.reshape(ep, CAPACITY, width), "ep", 0, 0, tiled=True)
    return combine(returned.reshape(ep * CAPACITY, width), routes, scores)


def on_device(x, valve, taps, carry, entry, lane, jump, tok, scale, routes, scores, expand, contract):
    mixed = temporal(x, valve, taps, carry, entry, lane, jump)
    return (mixed, expert(tok, scale, routes, scores, expand, contract))


def solution(mesh):
    rows = P(("grp", "ep"), None)
    split = P(("grp", "ep"), "tp")
    placed = (
        split,
        split,
        P(None, "tp"),
        P("tp", None, None),
        P("tp", None, None),
        P("tp"),
        P(("grp", "ep")),
        rows,
        P(),
        rows,
        rows,
        P("ep", None, "tp"),
        P("ep", None, "tp"),
    )
    return jax.shard_map(
        on_device, mesh=mesh, in_specs=placed, out_specs=(split, split), check_vma=False
    )
```

```python
import functools

import jax
import jax.numpy as jnp
from jax import lax
from jax.experimental import pallas as pl
from jax.experimental.pallas import tpu as pltpu
from jax.sharding import PartitionSpec as P

CONV = 4
CAPACITY = 24
F32 = jnp.float32
BF16 = jnp.bfloat16

NN = (((1,), (0,)), ((), ()))
NT = (((1,), (1,)), ((), ()))


def dot(a, b, dims=NN):
    return lax.dot_general(a, b, dims, preferred_element_type=F32)


def vmem():
    return pl.BlockSpec(memory_space=pltpu.VMEM)


def smem():
    return pl.BlockSpec(memory_space=pltpu.SMEM)


def cost(flops, nbytes):
    return pl.CostEstimate(flops=flops, bytes_accessed=nbytes, transcendentals=0)


def grant(mebibytes):
    return pltpu.CompilerParams(vmem_limit_bytes=mebibytes * 2**20)


def same(shape, offset=0):
    rows = lax.broadcasted_iota(jnp.int32, shape, 0)
    return (rows + offset == lax.broadcasted_iota(jnp.int32, shape, 1)).astype(F32)


def dispatch_kernel(at_ref, tok_ref, scale_ref, routes_ref, out_ref):
    tokens, features = tok_ref.shape
    slots, width = out_ref.shape
    experts = slots // CAPACITY
    first = pl.multiple_of(at_ref[0] * width, width)
    rows = tok_ref[...].astype(F32)
    mean = jnp.sum(rows, axis=1, keepdims=True) * (1.0 / features)
    centered = rows - mean
    var = jnp.sum(centered * centered, axis=1, keepdims=True) * (1.0 / features)
    part = tok_ref[:, pl.ds(first, width)].astype(F32) - mean
    normed = (part * lax.rsqrt(var + 1e-05) * scale_ref[:, pl.ds(first, width)]).astype(BF16)
    ranks = lax.broadcasted_iota(jnp.int32, (experts, tokens), 0)
    named = [(routes_ref[k : k + 1, :] == ranks).astype(F32) for k in range(2)]
    earlier = (
        lax.broadcasted_iota(jnp.int32, (tokens, tokens), 0)
        < lax.broadcasted_iota(jnp.int32, (tokens, tokens), 1)
    ).astype(F32).astype(BF16)
    place = ranks.astype(F32) * CAPACITY + dot((named[0] + named[1]).astype(BF16), earlier)
    slot = [jnp.sum(m * place, axis=0, keepdims=True).astype(jnp.int32) for m in named]
    ids = lax.broadcasted_iota(jnp.int32, (slots, tokens), 0)
    pick = jnp.logical_or(ids == slot[0], ids == slot[1]).astype(F32).astype(BF16)
    out_ref[...] = dot(pick, normed).astype(BF16)


def dispatch(tok, scale, routes, at, experts, width):
    slots = experts * CAPACITY
    return pl.pallas_call(
        dispatch_kernel,
        out_shape=jax.ShapeDtypeStruct((slots, width), BF16),
        in_specs=[smem(), vmem(), vmem(), vmem()],
        out_specs=vmem(),
        cost_estimate=cost(2 * slots * tok.shape[0] * width, 2 * tok.size + 2 * slots * width),
        name="dispatch",
    )(at, tok, scale, routes)


def combined(ret_ref, routes_ref, score_ref, rows_ref):
    experts = ret_ref.shape[0]
    slots, width = rows_ref.shape
    tokens = routes_ref.shape[0]
    lanes = width // 2
    for e in range(experts):
        for h in range(2):
            part = ret_ref[e, h * CAPACITY : (h + 1) * CAPACITY, :].astype(F32)
            rows_ref[e * CAPACITY : (e + 1) * CAPACITY, h * lanes : (h + 1) * lanes] = part
    rows = rows_ref[...].astype(BF16)
    ranks = lax.broadcasted_iota(jnp.int32, (tokens, experts), 1)
    hot = [(routes_ref[:, k : k + 1] == ranks).astype(F32) for k in range(2)]
    earlier = (
        lax.broadcasted_iota(jnp.int32, (tokens, tokens), 1)
        < lax.broadcasted_iota(jnp.int32, (tokens, tokens), 0)
    ).astype(F32).astype(BF16)
    place = ranks.astype(F32) * CAPACITY + dot(earlier, (hot[0] + hot[1]).astype(BF16))
    ids = lax.broadcasted_iota(jnp.int32, (tokens, slots), 1)
    picked = []
    for m in hot:
        slot = jnp.sum(m * place, axis=1, keepdims=True).astype(jnp.int32)
        picked.append(dot((ids == slot).astype(F32).astype(BF16), rows))
    weight = jax.nn.sigmoid(score_ref[:, 0:1] - score_ref[:, 1:2])
    return weight * picked[0] + (1.0 - weight) * picked[1]


def finish_kernel(at_ref, ret_ref, routes_ref, score_ref, decay_ref, state_ref, valve_ref, moe_ref, mix_ref, rows_ref):
    moe_ref[...] = combined(ret_ref, routes_ref, score_ref, rows_ref).astype(BF16)
    length, channels = state_ref.shape
    me = at_ref[0]
    entering = jnp.zeros((1, 256), F32)
    for d in range(ret_ref.shape[0]):
        ends = ret_ref[d, 2 * CAPACITY : 2 * CAPACITY + 8, :].astype(F32)
        wide = [
            jnp.concatenate([ends[k : k + 1] + ends[k + 1 : k + 2], ends[k + 4 : k + 5] + ends[k + 5 : k + 6]], axis=1)
            for k in (0, 2)
        ]
        entering = jnp.where(d < me, wide[0] * entering + wide[1], entering)
    state = state_ref[...] + decay_ref[...] * entering[:, 0:channels]
    valve = dot(same((length, length)).astype(BF16), valve_ref[...], NT)
    mixed = (state * jax.nn.gelu(valve, approximate=True)).astype(BF16)
    mix_ref[...] = dot(same((channels, channels)).astype(BF16), mixed, NT).astype(BF16)


def finish(returned, routes, scores, decay, state, valve, at):
    slots = returned.shape[0] * CAPACITY
    width = 2 * returned.shape[2]
    tokens = routes.shape[0]
    return pl.pallas_call(
        finish_kernel,
        out_shape=(
            jax.ShapeDtypeStruct((tokens, width), BF16),
            jax.ShapeDtypeStruct(valve.shape, BF16),
        ),
        in_specs=[smem()] + [vmem()] * 6,
        out_specs=(vmem(), vmem()),
        scratch_shapes=[pltpu.VMEM((slots, width), F32)],
        cost_estimate=cost(4 * slots * tokens * width, 4 * slots * width),
        compiler_params=grant(12),
        name="finish",
    )(at, returned, routes, scores, decay, state, valve)


def ring(block, axis, beside):
    size = lax.axis_size(axis)
    ahead = [(i, (i + 1) % size) for i in range(size)]
    back = [(i, (i - 1) % size) for i in range(size)]
    left = right = block
    pieces = [block]
    for _ in range(size // 2 - 1):
        left = lax.ppermute(left, axis, ahead)
        right = lax.ppermute(right, axis, back)
        pieces += [left, right]
    near, other, beside = lax.optimization_barrier((left[0], right[1], beside))
    far = (lax.ppermute(near, axis, ahead), lax.ppermute(other, axis, back))
    return pieces, far, beside


def steps_of(size):
    steps = [0]
    for s in range(1, size // 2):
        steps += [size - s, s]
    return steps + [size // 2]


def up_kernel(steps, size, first, last, at_ref, *refs):
    count = len(steps) - last
    pieces, refs = refs[:count], refs[count:]
    far, refs = (refs[:2], refs[2:]) if last else ((), refs)
    total_ref, refs = (None, refs) if first else (refs[0], refs[1:])
    w_ref, out_ref = refs
    width = pieces[0].shape[2]
    units = w_ref.shape[0]
    edge = units % 128
    even = units - edge

    def columns(k):
        owner = lax.rem(at_ref[0] + steps[k], size)
        return w_ref[:, pl.ds(pl.multiple_of(owner * width, width), width)]

    for side in range(2):
        total = None if first else total_ref[side]
        for k, piece in enumerate(pieces):
            term = dot(piece[side], columns(k), NT)
            total = term if total is None else total + term
        if last:
            total = total + dot(far[side][...], columns(count), NT)
            hidden = (total * jax.nn.sigmoid(total)).astype(BF16)
            out_ref[:, side * even : (side + 1) * even] = hidden[:, 0:even]
            at = 2 * even + side * edge
            out_ref[:, at : at + edge] = hidden[:, even:units]
        else:
            out_ref[side] = total


def down_kernel(steps, size, first, last, at_ref, *refs):
    count = len(steps) - last
    pieces, refs = refs[:count], refs[count:]
    far, refs = (refs[:2], refs[2:]) if last else ((), refs)
    total_ref, refs = (None, refs) if first else (refs[0], refs[1:])
    ends_ref, refs = (refs[0], refs[1:]) if last else (None, refs)
    w_ref, out_ref = refs
    rows, both = pieces[0].shape[1:]
    units = both // 2
    edge = units % 128
    even = units - edge

    def term(block, k, side):
        owner = lax.rem(at_ref[0] + steps[k], size)
        at = 2 * even + side * edge
        mine = jnp.concatenate(
            [block[:, side * even : (side + 1) * even], block[:, at : at + edge]], axis=1
        )
        return dot(mine, w_ref[pl.ds(pl.multiple_of(owner * units, 64), units), :])

    if last:
        tail = ends_ref[...].astype(BF16)
        for d in range(out_ref.shape[0]):
            out_ref[d, 2 * CAPACITY : 2 * CAPACITY + 8, :] = tail
    for side in range(2):
        for part in range(2):
            span = slice(part * rows, (part + 1) * rows)
            total = None if first else total_ref[side, span]
            for k, piece in enumerate(pieces):
                value = term(piece.at[part], k, side)
                total = value if total is None else total + value
            if not last:
                out_ref[side, span] = total
                continue
            total = (total + term(far[part], count, side)).astype(BF16)
            lanes = total.shape[1] // 2
            group = rows // CAPACITY
            for j in range(group):
                d = (side * 2 + part) * group + j
                mine = total[j * CAPACITY : (j + 1) * CAPACITY]
                out_ref[d, 0:CAPACITY, :] = mine[:, 0:lanes]
                out_ref[d, CAPACITY : 2 * CAPACITY, :] = mine[:, lanes:]


def stage(body, name, steps, pieces, rest, at, out):
    size = lax.axis_size("tp")
    first = len(rest) == 1
    operands = [*pieces, *rest]
    kernel = functools.partial(body, steps, size, first, not first)
    macs = len(steps) * pieces[0].size * rest[-1].size // pieces[0].shape[-1] // size
    moved = sum(v.size * v.dtype.itemsize for v in operands)
    return pl.pallas_call(
        kernel,
        out_shape=out,
        in_specs=[smem()] + [vmem()] * len(operands),
        out_specs=vmem(),
        cost_estimate=cost(2 * macs, moved),
        compiler_params=grant(20),
        name=name,
    )(at, *operands)


def staged(body, name, block, w, at, beside, middle, out, extra=()):
    pieces, far, beside = ring(block, "tp", beside)
    steps = steps_of(lax.axis_size("tp"))
    cut = len(pieces) - 2
    total = stage(body, name + "_near", steps[:cut], pieces[:cut], [w], at, middle)
    rest = [*far, total, *extra, w]
    return stage(body, name + "_far", steps[cut:], pieces[cut:], rest, at, out), beside


def up(block, w, at, beside):
    _, half, _ = block.shape
    units = w.shape[0]
    middle = jax.ShapeDtypeStruct((2, half, units), F32)
    out = jax.ShapeDtypeStruct((half, 2 * units), BF16)
    return staged(up_kernel, "up", block, w, at, beside, middle, out)


def down(block, w, at, ends):
    _, rows, _ = block.shape
    width = w.shape[1]
    middle = jax.ShapeDtypeStruct((2, 2 * rows, width), F32)
    out = jax.ShapeDtypeStruct((4 * rows // CAPACITY, 2 * CAPACITY + 8, width // 2), BF16)
    done, _ = staged(down_kernel, "down", block, w, at, (), middle, out, (ends,))
    return done


def one_minus_exp(y):
    small = -y * (1.0 + y * (0.5 + y * (1.0 / 6 + y * (1.0 / 24 + y * (1.0 / 120 + y / 720)))))
    return jnp.where(y > -0.25, small, 1.0 - jnp.exp(y))


def local_kernel(x_ref, prev_ref, tap_ref, carry_ref, entry_ref, lane_ref, jump_ref, decay_ref, state_ref, ends_ref, pad_ref):
    channels, length = x_ref.shape
    pad_ref[0:8, :] = dot(same((8, length), length - 8).astype(BF16), prev_ref[...], NT)
    pad_ref[8 : 8 + length, :] = dot(same((length, length)).astype(BF16), x_ref[...], NT)
    taps = tap_ref[...].astype(F32)
    conv = jnp.zeros((length, channels), F32)
    for j in range(CONV):
        at = 8 - (CONV - 1) + j
        conv = conv + pad_ref[at : at + length, :] * taps[j : j + 1]
    half = conv.astype(BF16)
    recur = jax.nn.sigmoid(dot(half, carry_ref[0]))
    entry = jax.nn.sigmoid(dot(half, entry_ref[0]))
    fade = jnp.exp(-lane_ref[...])
    series = fade * (1.0 - fade * (0.5 - fade * (1.0 / 3 - fade * (0.25 - fade * 0.2))))
    soft = jnp.where(fade < 0.03, series, jnp.log(1.0 + fade))
    jump = jnp.sum(same((length, length)) * jump_ref[...], axis=1, keepdims=True)
    log_decay = -8.0 * recur * soft + jump
    state = jnp.sqrt(one_minus_exp(2.0 * log_decay)) * entry * conv
    decay = jnp.exp(log_decay)
    rows = lax.broadcasted_iota(jnp.int32, (length, channels), 0)
    step = 1
    while step < length:
        ready = rows >= step
        before_state = jnp.where(ready, pltpu.roll(state, step, 0), 0.0)
        before_decay = jnp.where(ready, pltpu.roll(decay, step, 0), 1.0)
        state = decay * before_state + state
        decay = decay * before_decay
        step *= 2
    decay_ref[...] = decay
    state_ref[...] = state
    ends_ref[...] = jnp.zeros((8, 128), F32)
    for k, value in enumerate((decay[length - 1 : length], state[length - 1 : length])):
        high = value.astype(BF16).astype(F32)
        for j, term in enumerate((high, value - high)):
            r = 2 * k + j
            ends_ref[r : r + 1, :] = term[:, 0:128]
            ends_ref[r + 4 : r + 5, 0 : channels - 128] = term[:, 128:channels]


def local_scan(x, prev, taps, carry, entry, lane, jump):
    channels, length = x.shape
    full = jax.ShapeDtypeStruct((length, channels), F32)
    return pl.pallas_call(
        local_kernel,
        out_shape=(full, full, jax.ShapeDtypeStruct((8, 128), F32)),
        in_specs=[vmem()] * 7,
        out_specs=(vmem(), vmem(), vmem()),
        scratch_shapes=[pltpu.VMEM((length + 8, channels), F32)],
        cost_estimate=cost(100 * length * channels, 16 * length * channels),
        compiler_params=grant(6),
        name="local_scan",
    )(x, prev, taps, carry, entry, lane, jump)


def here(axis):
    return lax.axis_index(axis).astype(jnp.int32).reshape(1)


def on_device(x, valve, taps, carry, entry, lane, jump, tok, scale, routes, scores, expand, contract):
    ep = lax.axis_size("ep")
    width = tok.shape[1] // lax.axis_size("tp")
    at = here("tp")
    sent = dispatch(tok, scale[None, :], routes.T, at, ep, width)
    arrived = lax.all_to_all(sent.reshape(ep, CAPACITY, width), "ep", 0, 0, tiled=True)
    arrived, flipped = lax.optimization_barrier((arrived, x.T))
    prev = lax.ppermute(flipped, "ep", [(i, i + 1) for i in range(ep - 1)])
    local = local_scan(flipped, prev, taps, carry, entry, lane[None, :], jump[None, :])
    half = ep * CAPACITY // 2
    hidden, local = up(arrived.reshape(2, half, width), expand[0].T, at, local)
    decay, state, ends = local
    done = down(hidden.reshape(2, half // 2, -1), contract[0], at, ends)
    returned = lax.all_to_all(done, "ep", 0, 0, tiled=True)
    moe, mixed = finish(returned, routes, scores, decay, state, valve.T, here("ep"))
    return (mixed.T, moe)


def solution(mesh):
    rows = P(("grp", "ep"), None)
    split = P(("grp", "ep"), "tp")
    placed = (
        split,
        split,
        P(None, "tp"),
        P("tp", None, None),
        P("tp", None, None),
        P("tp"),
        P(("grp", "ep")),
        rows,
        P(),
        rows,
        rows,
        P("ep", None, "tp"),
        P("ep", None, "tp"),
    )
    return jax.shard_map(
        on_device, mesh=mesh, in_specs=placed, out_specs=(split, split), check_vma=False
    )
```

```python
import functools

import jax
import jax.numpy as jnp
from jax import lax
from jax.experimental import pallas as pl
from jax.experimental.pallas import tpu as pltpu
from jax.sharding import PartitionSpec as P

CONV = 4
CAPACITY = 24
F32 = jnp.float32
BF16 = jnp.bfloat16

NN = (((1,), (0,)), ((), ()))
NT = (((1,), (1,)), ((), ()))


def dot(a, b, dims=NN):
    return lax.dot_general(a, b, dims, preferred_element_type=F32)


def vmem():
    return pl.BlockSpec(memory_space=pltpu.VMEM)


def smem():
    return pl.BlockSpec(memory_space=pltpu.SMEM)


def cost(flops, nbytes):
    return pl.CostEstimate(flops=flops, bytes_accessed=nbytes, transcendentals=0)


def grant(mebibytes):
    return pltpu.CompilerParams(vmem_limit_bytes=mebibytes * 2**20)


def same(shape, offset=0):
    rows = lax.broadcasted_iota(jnp.int32, shape, 0)
    return (rows + offset == lax.broadcasted_iota(jnp.int32, shape, 1)).astype(F32)


def dispatch_kernel(at_ref, tok_ref, scale_ref, routes_ref, out_ref):
    tokens, features = tok_ref.shape
    slots, width = out_ref.shape
    experts = slots // CAPACITY
    first = pl.multiple_of(at_ref[0] * width, width)
    rows = tok_ref[...].astype(F32)
    mean = jnp.sum(rows, axis=1, keepdims=True) * (1.0 / features)
    centered = rows - mean
    var = jnp.sum(centered * centered, axis=1, keepdims=True) * (1.0 / features)
    part = tok_ref[:, pl.ds(first, width)].astype(F32) - mean
    normed = (part * lax.rsqrt(var + 1e-05) * scale_ref[:, pl.ds(first, width)]).astype(BF16)
    ranks = lax.broadcasted_iota(jnp.int32, (experts, tokens), 0)
    named = [(routes_ref[k : k + 1, :] == ranks).astype(F32) for k in range(2)]
    earlier = (
        lax.broadcasted_iota(jnp.int32, (tokens, tokens), 0)
        < lax.broadcasted_iota(jnp.int32, (tokens, tokens), 1)
    ).astype(F32).astype(BF16)
    place = ranks.astype(F32) * CAPACITY + dot((named[0] + named[1]).astype(BF16), earlier)
    slot = [jnp.sum(m * place, axis=0, keepdims=True).astype(jnp.int32) for m in named]
    ids = lax.broadcasted_iota(jnp.int32, (slots, tokens), 0)
    pick = jnp.logical_or(ids == slot[0], ids == slot[1]).astype(F32).astype(BF16)
    out_ref[...] = dot(pick, normed).astype(BF16)


def dispatch(tok, scale, routes, at, experts, width):
    slots = experts * CAPACITY
    return pl.pallas_call(
        dispatch_kernel,
        out_shape=jax.ShapeDtypeStruct((slots, width), BF16),
        in_specs=[smem(), vmem(), vmem(), vmem()],
        out_specs=vmem(),
        cost_estimate=cost(2 * slots * tok.shape[0] * width, 2 * tok.size + 2 * slots * width),
        name="dispatch",
    )(at, tok, scale, routes)


def combined(ret_ref, routes_ref, score_ref, rows_ref):
    experts = ret_ref.shape[0]
    slots, width = rows_ref.shape
    tokens = routes_ref.shape[0]
    lanes = width // 2
    for e in range(experts):
        for h in range(2):
            part = ret_ref[e, h * CAPACITY : (h + 1) * CAPACITY, :].astype(F32)
            rows_ref[e * CAPACITY : (e + 1) * CAPACITY, h * lanes : (h + 1) * lanes] = part
    rows = rows_ref[...].astype(BF16)
    ranks = lax.broadcasted_iota(jnp.int32, (tokens, experts), 1)
    hot = [(routes_ref[:, k : k + 1] == ranks).astype(F32) for k in range(2)]
    earlier = (
        lax.broadcasted_iota(jnp.int32, (tokens, tokens), 1)
        < lax.broadcasted_iota(jnp.int32, (tokens, tokens), 0)
    ).astype(F32).astype(BF16)
    place = ranks.astype(F32) * CAPACITY + dot(earlier, (hot[0] + hot[1]).astype(BF16))
    ids = lax.broadcasted_iota(jnp.int32, (tokens, slots), 1)
    picked = []
    for m in hot:
        slot = jnp.sum(m * place, axis=1, keepdims=True).astype(jnp.int32)
        picked.append(dot((ids == slot).astype(F32).astype(BF16), rows))
    weight = jax.nn.sigmoid(score_ref[:, 0:1] - score_ref[:, 1:2])
    return weight * picked[0] + (1.0 - weight) * picked[1]


def finish_kernel(at_ref, ret_ref, routes_ref, score_ref, decay_ref, state_ref, valve_ref, moe_ref, mix_ref, rows_ref):
    moe_ref[...] = combined(ret_ref, routes_ref, score_ref, rows_ref).astype(BF16)
    length, channels = state_ref.shape
    me = at_ref[0]
    entering = jnp.zeros((1, 256), F32)
    for d in range(ret_ref.shape[0]):
        ends = ret_ref[d, 2 * CAPACITY : 2 * CAPACITY + 8, :].astype(F32)
        wide = [
            jnp.concatenate([ends[k : k + 1] + ends[k + 1 : k + 2], ends[k + 4 : k + 5] + ends[k + 5 : k + 6]], axis=1)
            for k in (0, 2)
        ]
        entering = jnp.where(d < me, wide[0] * entering + wide[1], entering)
    state = state_ref[...] + decay_ref[...] * entering[:, 0:channels]
    valve = dot(same((length, length)).astype(BF16), valve_ref[...], NT)
    mixed = (state * jax.nn.gelu(valve, approximate=True)).astype(BF16)
    mix_ref[...] = dot(same((channels, channels)).astype(BF16), mixed, NT).astype(BF16)


def finish(returned, routes, scores, decay, state, valve, at):
    slots = returned.shape[0] * CAPACITY
    width = 2 * returned.shape[2]
    tokens = routes.shape[0]
    return pl.pallas_call(
        finish_kernel,
        out_shape=(
            jax.ShapeDtypeStruct((tokens, width), BF16),
            jax.ShapeDtypeStruct(valve.shape, BF16),
        ),
        in_specs=[smem()] + [vmem()] * 6,
        out_specs=(vmem(), vmem()),
        scratch_shapes=[pltpu.VMEM((slots, width), F32)],
        cost_estimate=cost(4 * slots * tokens * width, 4 * slots * width),
        compiler_params=grant(12),
        name="finish",
    )(at, returned, routes, scores, decay, state, valve)


def mirrored(block, sense):
    ep = lax.axis_size("ep")
    tp = lax.axis_size("tp")
    route = []
    for e in range(ep):
        turn = sense if e % 2 == 0 else -sense
        route += [(e * tp + t, e * tp + (t + turn) % tp) for t in range(tp)]
    return lax.ppermute(block, ("ep", "tp"), route)


def ring(block, holds):
    size = lax.axis_size("tp")
    first = second = block
    pieces = [block]
    for hop in range(size // 2 - 1):
        if hop in holds:
            second = holds[hop](second)
        first = mirrored(first, 1)
        second = mirrored(second, -1)
        pieces += [first, second]
    return pieces, mirrored(first, 1)


def steps_of(size):
    steps = [0]
    for s in range(1, size // 2):
        steps += [s, -s]
    return steps + [size // 2]


def owner_of(tp_ref, ep_ref, step, size):
    return lax.rem(tp_ref[0] + size + step * (2 * lax.rem(ep_ref[0], 2) - 1), size)


def up_kernel(steps, size, first, tp_ref, ep_ref, *refs):
    pieces, refs = refs[: len(steps)], refs[len(steps) :]
    total_ref, refs = (None, refs) if first else (refs[0], refs[1:])
    w_ref, out_ref = refs
    width = pieces[0].shape[2]
    units = w_ref.shape[0]
    edge = units % 128
    even = units - edge

    def columns(step):
        owner = owner_of(tp_ref, ep_ref, step, size)
        return w_ref[:, pl.ds(pl.multiple_of(owner * width, width), width)]

    for side in range(2):
        total = None if first else total_ref[side]
        for step, piece in zip(steps, pieces):
            term = dot(piece[side], columns(step), NT)
            total = term if total is None else total + term
        if first:
            out_ref[side] = total
            continue
        hidden = (total * jax.nn.sigmoid(total)).astype(BF16)
        out_ref[:, side * even : (side + 1) * even] = hidden[:, 0:even]
        at = 2 * even + side * edge
        out_ref[:, at : at + edge] = hidden[:, even:units]


def down_kernel(steps, size, first, tp_ref, ep_ref, *refs):
    pieces, refs = refs[: len(steps)], refs[len(steps) :]
    total_ref, ends_ref, refs = (None, None, refs) if first else (*refs[:2], refs[2:])
    w_ref, out_ref = refs
    rows, both = pieces[0].shape[1:]
    units = both // 2
    edge = units % 128
    even = units - edge

    def term(block, step, side):
        owner = owner_of(tp_ref, ep_ref, step, size)
        at = 2 * even + side * edge
        mine = jnp.concatenate(
            [block[:, side * even : (side + 1) * even], block[:, at : at + edge]], axis=1
        )
        return dot(mine, w_ref[pl.ds(pl.multiple_of(owner * units, 64), units), :])

    if not first:
        tail = ends_ref[...].astype(BF16)
        for d in range(out_ref.shape[0]):
            out_ref[d, 2 * CAPACITY : 2 * CAPACITY + 8, :] = tail
    for side in range(2):
        for part in range(2):
            span = slice(part * rows, (part + 1) * rows)
            total = None if first else total_ref[side, span]
            for step, piece in zip(steps, pieces):
                value = term(piece.at[part], step, side)
                total = value if total is None else total + value
            if first:
                out_ref[side, span] = total
                continue
            total = total.astype(BF16)
            lanes = total.shape[1] // 2
            group = rows // CAPACITY
            for j in range(group):
                d = (side * 2 + part) * group + j
                mine = total[j * CAPACITY : (j + 1) * CAPACITY]
                out_ref[d, 0:CAPACITY, :] = mine[:, 0:lanes]
                out_ref[d, CAPACITY : 2 * CAPACITY, :] = mine[:, lanes:]


def stage(body, name, steps, pieces, rest, at, out):
    size = lax.axis_size("tp")
    operands = [*pieces, *rest]
    kernel = functools.partial(body, steps, size, len(rest) == 1)
    macs = len(steps) * pieces[0].size * rest[-1].size // pieces[0].shape[-1] // size
    moved = sum(v.size * v.dtype.itemsize for v in operands)
    return pl.pallas_call(
        kernel,
        out_shape=out,
        in_specs=[smem()] * 2 + [vmem()] * len(operands),
        out_specs=vmem(),
        cost_estimate=cost(2 * macs, moved),
        compiler_params=grant(20),
        name=name,
    )(*at, *operands)


def staged(body, name, block, w, at, holds, middle, out, extra=()):
    pieces, far = ring(block, holds)
    steps = steps_of(lax.axis_size("tp"))
    total = stage(body, name + "_near", steps[:-1], pieces, [w], at, middle)
    return stage(body, name + "_far", steps[-1:], [far], [total, *extra, w], at, out)


def up(block, w, at, holds):
    _, half, _ = block.shape
    units = w.shape[0]
    middle = jax.ShapeDtypeStruct((2, half, units), F32)
    out = jax.ShapeDtypeStruct((half, 2 * units), BF16)
    return staged(up_kernel, "up", block, w, at, holds, middle, out)


def down(block, w, at, ends):
    _, rows, _ = block.shape
    width = w.shape[1]
    middle = jax.ShapeDtypeStruct((2, 2 * rows, width), F32)
    out = jax.ShapeDtypeStruct((4 * rows // CAPACITY, 2 * CAPACITY + 8, width // 2), BF16)
    return staged(down_kernel, "down", block, w, at, {}, middle, out, (ends,))


def one_minus_exp(y):
    small = -y * (1.0 + y * (0.5 + y * (1.0 / 6 + y * (1.0 / 24 + y * (1.0 / 120 + y / 720)))))
    return jnp.where(y > -0.25, small, 1.0 - jnp.exp(y))


def local_kernel(x_ref, prev_ref, tap_ref, carry_ref, entry_ref, lane_ref, jump_ref, decay_ref, state_ref, ends_ref, pad_ref):
    channels, length = x_ref.shape
    pad_ref[0:8, :] = dot(same((8, length), length - 8).astype(BF16), prev_ref[...], NT)
    pad_ref[8 : 8 + length, :] = dot(same((length, length)).astype(BF16), x_ref[...], NT)
    taps = tap_ref[...].astype(F32)
    conv = jnp.zeros((length, channels), F32)
    for j in range(CONV):
        at = 8 - (CONV - 1) + j
        conv = conv + pad_ref[at : at + length, :] * taps[j : j + 1]
    half = conv.astype(BF16)
    recur = jax.nn.sigmoid(dot(half, carry_ref[0]))
    entry = jax.nn.sigmoid(dot(half, entry_ref[0]))
    fade = jnp.exp(-lane_ref[...])
    series = fade * (1.0 - fade * (0.5 - fade * (1.0 / 3 - fade * (0.25 - fade * 0.2))))
    soft = jnp.where(fade < 0.03, series, jnp.log(1.0 + fade))
    jump = jnp.sum(same((length, length)) * jump_ref[...], axis=1, keepdims=True)
    log_decay = -8.0 * recur * soft + jump
    state = jnp.sqrt(one_minus_exp(2.0 * log_decay)) * entry * conv
    decay = jnp.exp(log_decay)
    rows = lax.broadcasted_iota(jnp.int32, (length, channels), 0)
    step = 1
    while step < length:
        ready = rows >= step
        before_state = jnp.where(ready, pltpu.roll(state, step, 0), 0.0)
        before_decay = jnp.where(ready, pltpu.roll(decay, step, 0), 1.0)
        state = decay * before_state + state
        decay = decay * before_decay
        step *= 2
    decay_ref[...] = decay
    state_ref[...] = state
    ends_ref[...] = jnp.zeros((8, 128), F32)
    for k, value in enumerate((decay[length - 1 : length], state[length - 1 : length])):
        high = value.astype(BF16).astype(F32)
        for j, term in enumerate((high, value - high)):
            r = 2 * k + j
            ends_ref[r : r + 1, :] = term[:, 0:128]
            ends_ref[r + 4 : r + 5, 0 : channels - 128] = term[:, 128:channels]


def local_scan(x, prev, taps, carry, entry, lane, jump):
    channels, length = x.shape
    full = jax.ShapeDtypeStruct((length, channels), F32)
    return pl.pallas_call(
        local_kernel,
        out_shape=(full, full, jax.ShapeDtypeStruct((8, 128), F32)),
        in_specs=[vmem()] * 7,
        out_specs=(vmem(), vmem(), vmem()),
        scratch_shapes=[pltpu.VMEM((length + 8, channels), F32)],
        cost_estimate=cost(100 * length * channels, 16 * length * channels),
        compiler_params=grant(6),
        name="local_scan",
    )(x, prev, taps, carry, entry, lane, jump)


def here(axis):
    return lax.axis_index(axis).astype(jnp.int32).reshape(1)


def on_device(x, valve, taps, carry, entry, lane, jump, tok, scale, routes, scores, expand, contract):
    ep = lax.axis_size("ep")
    width = tok.shape[1] // lax.axis_size("tp")
    at = (here("tp"), here("ep"))
    sent = dispatch(tok, scale[None, :], routes.T, at[0], ep, width)
    arrived = lax.all_to_all(sent.reshape(ep, CAPACITY, width), "ep", 0, 0, tiled=True)
    arrived, flipped = lax.optimization_barrier((arrived, x.T))
    prev = lax.ppermute(flipped, "ep", [(i, i + 1) for i in range(ep - 1)])
    kept = {}

    def hold_prev(block):
        block, kept["prev"] = lax.optimization_barrier((block, prev))
        return block

    def hold_scan(block):
        local = local_scan(flipped, kept["prev"], taps, carry, entry, lane[None, :], jump[None, :])
        block, kept["local"] = lax.optimization_barrier((block, local))
        return block

    half = ep * CAPACITY // 2
    blocks = arrived.reshape(2, half, width)
    hidden = up(blocks, expand[0].T, at, {1: hold_prev, 2: hold_scan})
    decay, state, ends = kept["local"]
    done = down(hidden.reshape(2, half // 2, -1), contract[0], at, ends)
    returned = lax.all_to_all(done, "ep", 0, 0, tiled=True)
    moe, mixed = finish(returned, routes, scores, decay, state, valve.T, at[1])
    return (mixed.T, moe)


def solution(mesh):
    rows = P(("grp", "ep"), None)
    split = P(("grp", "ep"), "tp")
    placed = (
        split,
        split,
        P(None, "tp"),
        P("tp", None, None),
        P("tp", None, None),
        P("tp"),
        P(("grp", "ep")),
        rows,
        P(),
        rows,
        rows,
        P("ep", None, "tp"),
        P("ep", None, "tp"),
    )
    return jax.shard_map(
        on_device, mesh=mesh, in_specs=placed, out_specs=(split, split), check_vma=False
    )
```

```python
import functools

import jax
import jax.numpy as jnp
from jax import lax
from jax.experimental import pallas as pl
from jax.experimental.pallas import tpu as pltpu
from jax.sharding import PartitionSpec as P

CONV = 4
CAPACITY = 24
F32 = jnp.float32
BF16 = jnp.bfloat16

NN = (((1,), (0,)), ((), ()))
NT = (((1,), (1,)), ((), ()))


def dot(a, b, dims=NN):
    return lax.dot_general(a, b, dims, preferred_element_type=F32)


def vmem():
    return pl.BlockSpec(memory_space=pltpu.VMEM)


def smem():
    return pl.BlockSpec(memory_space=pltpu.SMEM)


def cost(flops, nbytes):
    return pl.CostEstimate(flops=flops, bytes_accessed=nbytes, transcendentals=0)


def grant(mebibytes):
    return pltpu.CompilerParams(vmem_limit_bytes=mebibytes * 2**20)


def same(shape, offset=0):
    rows = lax.broadcasted_iota(jnp.int32, shape, 0)
    return (rows + offset == lax.broadcasted_iota(jnp.int32, shape, 1)).astype(F32)


def dispatch_kernel(at_ref, tok_ref, scale_ref, routes_ref, out_ref):
    tokens, features = tok_ref.shape
    slots, width = out_ref.shape
    experts = slots // CAPACITY
    first = pl.multiple_of(at_ref[0] * width, width)
    rows = tok_ref[...].astype(F32)
    mean = jnp.sum(rows, axis=1, keepdims=True) * (1.0 / features)
    centered = rows - mean
    var = jnp.sum(centered * centered, axis=1, keepdims=True) * (1.0 / features)
    part = tok_ref[:, pl.ds(first, width)].astype(F32) - mean
    normed = (part * lax.rsqrt(var + 1e-05) * scale_ref[:, pl.ds(first, width)]).astype(BF16)
    ranks = lax.broadcasted_iota(jnp.int32, (experts, tokens), 0)
    named = [(routes_ref[k : k + 1, :] == ranks).astype(F32) for k in range(2)]
    earlier = (
        lax.broadcasted_iota(jnp.int32, (tokens, tokens), 0)
        < lax.broadcasted_iota(jnp.int32, (tokens, tokens), 1)
    ).astype(F32).astype(BF16)
    place = ranks.astype(F32) * CAPACITY + dot((named[0] + named[1]).astype(BF16), earlier)
    slot = [jnp.sum(m * place, axis=0, keepdims=True).astype(jnp.int32) for m in named]
    ids = lax.broadcasted_iota(jnp.int32, (slots, tokens), 0)
    pick = jnp.logical_or(ids == slot[0], ids == slot[1]).astype(F32).astype(BF16)
    out_ref[...] = dot(pick, normed).astype(BF16)


def dispatch(tok, scale, routes, at, experts, width):
    slots = experts * CAPACITY
    return pl.pallas_call(
        dispatch_kernel,
        out_shape=jax.ShapeDtypeStruct((slots, width), BF16),
        in_specs=[smem(), vmem(), vmem(), vmem()],
        out_specs=vmem(),
        cost_estimate=cost(2 * slots * tok.shape[0] * width, 2 * tok.size + 2 * slots * width),
        name="dispatch",
    )(at, tok, scale, routes)


def combined(ret_ref, routes_ref, score_ref, rows_ref):
    experts = ret_ref.shape[0]
    slots, width = rows_ref.shape
    tokens = routes_ref.shape[0]
    lanes = width // 2
    for e in range(experts):
        for h in range(2):
            part = ret_ref[e, h * CAPACITY : (h + 1) * CAPACITY, :].astype(F32)
            rows_ref[e * CAPACITY : (e + 1) * CAPACITY, h * lanes : (h + 1) * lanes] = part
    rows = rows_ref[...].astype(BF16)
    ranks = lax.broadcasted_iota(jnp.int32, (tokens, experts), 1)
    hot = [(routes_ref[:, k : k + 1] == ranks).astype(F32) for k in range(2)]
    earlier = (
        lax.broadcasted_iota(jnp.int32, (tokens, tokens), 1)
        < lax.broadcasted_iota(jnp.int32, (tokens, tokens), 0)
    ).astype(F32).astype(BF16)
    place = ranks.astype(F32) * CAPACITY + dot(earlier, (hot[0] + hot[1]).astype(BF16))
    ids = lax.broadcasted_iota(jnp.int32, (tokens, slots), 1)
    picked = []
    for m in hot:
        slot = jnp.sum(m * place, axis=1, keepdims=True).astype(jnp.int32)
        picked.append(dot((ids == slot).astype(F32).astype(BF16), rows))
    weight = jax.nn.sigmoid(score_ref[:, 0:1] - score_ref[:, 1:2])
    return weight * picked[0] + (1.0 - weight) * picked[1]


def finish_kernel(at_ref, ret_ref, routes_ref, score_ref, decay_ref, state_ref, valve_ref, moe_ref, mix_ref, rows_ref):
    moe_ref[...] = combined(ret_ref, routes_ref, score_ref, rows_ref).astype(BF16)
    length, channels = state_ref.shape
    me = at_ref[0]
    entering = jnp.zeros((1, 256), F32)
    for d in range(ret_ref.shape[0]):
        ends = ret_ref[d, 2 * CAPACITY : 2 * CAPACITY + 8, :].astype(F32)
        wide = [
            jnp.concatenate([ends[k : k + 1] + ends[k + 1 : k + 2], ends[k + 4 : k + 5] + ends[k + 5 : k + 6]], axis=1)
            for k in (0, 2)
        ]
        entering = jnp.where(d < me, wide[0] * entering + wide[1], entering)
    state = state_ref[...] + decay_ref[...] * entering[:, 0:channels]
    valve = dot(same((length, length)).astype(BF16), valve_ref[...], NT)
    mixed = (state * jax.nn.gelu(valve, approximate=True)).astype(BF16)
    mix_ref[...] = dot(same((channels, channels)).astype(BF16), mixed, NT).astype(BF16)


def finish(returned, routes, scores, decay, state, valve, at):
    slots = returned.shape[0] * CAPACITY
    width = 2 * returned.shape[2]
    tokens = routes.shape[0]
    return pl.pallas_call(
        finish_kernel,
        out_shape=(
            jax.ShapeDtypeStruct((tokens, width), BF16),
            jax.ShapeDtypeStruct(valve.shape, BF16),
        ),
        in_specs=[smem()] + [vmem()] * 6,
        out_specs=(vmem(), vmem()),
        scratch_shapes=[pltpu.VMEM((slots, width), F32)],
        cost_estimate=cost(4 * slots * tokens * width, 4 * slots * width),
        compiler_params=grant(12),
        name="finish",
    )(at, returned, routes, scores, decay, state, valve)


def mirrored(block, sense):
    ep = lax.axis_size("ep")
    tp = lax.axis_size("tp")
    route = []
    for e in range(ep):
        turn = sense if e % 2 == 0 else -sense
        route += [(e * tp + t, e * tp + (t + turn) % tp) for t in range(tp)]
    return lax.ppermute(block, ("ep", "tp"), route)


def ring(block, holds):
    size = lax.axis_size("tp")
    first = second = block
    pieces = [block]
    for hop in range(size // 2 - 1):
        if hop in holds:
            second = holds[hop](second)
        first = mirrored(first, 1)
        second = mirrored(second, -1)
        pieces += [first, second]
    return pieces, [mirrored(first, 1)]


def plain_ring(block, holds):
    size = lax.axis_size("tp")
    ahead = [(i, (i + 1) % size) for i in range(size)]
    back = [(i, (i - 1) % size) for i in range(size)]
    first = second = block
    pieces = [block]
    for _ in range(size // 2 - 1):
        first = lax.ppermute(first, "tp", ahead)
        second = lax.ppermute(second, "tp", back)
        pieces += [first, second]
    return pieces, [lax.ppermute(first[0], "tp", ahead), lax.ppermute(second[1], "tp", back)]


def steps_of(size):
    steps = [0]
    for s in range(1, size // 2):
        steps += [s, -s]
    return steps + [size // 2]


def owner_of(tp_ref, ep_ref, step, size):
    return lax.rem(tp_ref[0] + size + step * (2 * lax.rem(ep_ref[0], 2) - 1), size)


def up_kernel(steps, size, first, tp_ref, ep_ref, *refs):
    pieces, refs = refs[: len(steps)], refs[len(steps) :]
    total_ref, refs = (None, refs) if first else (refs[0], refs[1:])
    w_ref, out_ref = refs
    width = pieces[0].shape[2]
    units = w_ref.shape[0]
    edge = units % 128
    even = units - edge

    def columns(step):
        owner = owner_of(tp_ref, ep_ref, step, size)
        return w_ref[:, pl.ds(pl.multiple_of(owner * width, width), width)]

    for side in range(2):
        total = None if first else total_ref[side]
        for step, piece in zip(steps, pieces):
            term = dot(piece[side], columns(step), NT)
            total = term if total is None else total + term
        if first:
            out_ref[side] = total
            continue
        hidden = (total * jax.nn.sigmoid(total)).astype(BF16)
        out_ref[:, side * even : (side + 1) * even] = hidden[:, 0:even]
        at = 2 * even + side * edge
        out_ref[:, at : at + edge] = hidden[:, even:units]


def down_kernel(steps, size, first, tp_ref, ep_ref, *refs):
    if first:
        pieces, total_ref, ends_ref = refs[: len(steps)], None, None
        blocks = [[piece.at[part] for piece in pieces] for part in range(2)]
    else:
        total_ref, ends_ref = refs[2:4]
        blocks = [[refs[0]], [refs[1]]]
    w_ref, out_ref = refs[-2:]
    rows, both = blocks[0][0].shape
    units = both // 2
    edge = units % 128
    even = units - edge

    def term(block, step, side):
        owner = lax.rem(tp_ref[0] + size - step, size)
        at = 2 * even + side * edge
        mine = jnp.concatenate(
            [block[:, side * even : (side + 1) * even], block[:, at : at + edge]], axis=1
        )
        return dot(mine, w_ref[pl.ds(pl.multiple_of(owner * units, 64), units), :])

    if not first:
        tail = ends_ref[...].astype(BF16)
        for d in range(out_ref.shape[0]):
            out_ref[d, 2 * CAPACITY : 2 * CAPACITY + 8, :] = tail
    for side in range(2):
        for part in range(2):
            span = slice(part * rows, (part + 1) * rows)
            total = None if first else total_ref[side, span]
            for step, block in zip(steps, blocks[part]):
                value = term(block, step, side)
                total = value if total is None else total + value
            if first:
                out_ref[side, span] = total
                continue
            total = total.astype(BF16)
            lanes = total.shape[1] // 2
            group = rows // CAPACITY
            for j in range(group):
                d = (side * 2 + part) * group + j
                mine = total[j * CAPACITY : (j + 1) * CAPACITY]
                out_ref[d, 0:CAPACITY, :] = mine[:, 0:lanes]
                out_ref[d, CAPACITY : 2 * CAPACITY, :] = mine[:, lanes:]


def stage(body, name, steps, pieces, rest, at, out):
    size = lax.axis_size("tp")
    operands = [*pieces, *rest]
    kernel = functools.partial(body, steps, size, len(rest) == 1)
    macs = len(steps) * pieces[0].size * rest[-1].size // pieces[0].shape[-1] // size
    moved = sum(v.size * v.dtype.itemsize for v in operands)
    return pl.pallas_call(
        kernel,
        out_shape=out,
        in_specs=[smem()] * 2 + [vmem()] * len(operands),
        out_specs=vmem(),
        cost_estimate=cost(2 * macs, moved),
        compiler_params=grant(20),
        name=name,
    )(*at, *operands)


def staged(body, name, way, block, w, at, holds, middle, out, extra=()):
    pieces, far = way(block, holds)
    steps = steps_of(lax.axis_size("tp"))
    total = stage(body, name + "_near", steps[:-1], pieces, [w], at, middle)
    return stage(body, name + "_far", steps[-1:], far, [total, *extra, w], at, out)


def up(block, w, at, holds):
    _, half, _ = block.shape
    units = w.shape[0]
    middle = jax.ShapeDtypeStruct((2, half, units), F32)
    out = jax.ShapeDtypeStruct((half, 2 * units), BF16)
    return staged(up_kernel, "up", ring, block, w, at, holds, middle, out)


def down(block, w, at, ends):
    _, rows, _ = block.shape
    width = w.shape[1]
    middle = jax.ShapeDtypeStruct((2, 2 * rows, width), F32)
    out = jax.ShapeDtypeStruct((4 * rows // CAPACITY, 2 * CAPACITY + 8, width // 2), BF16)
    return staged(down_kernel, "down", plain_ring, block, w, at, {}, middle, out, (ends,))


def one_minus_exp(y):
    small = -y * (1.0 + y * (0.5 + y * (1.0 / 6 + y * (1.0 / 24 + y * (1.0 / 120 + y / 720)))))
    return jnp.where(y > -0.25, small, 1.0 - jnp.exp(y))


def local_kernel(x_ref, prev_ref, tap_ref, carry_ref, entry_ref, lane_ref, jump_ref, decay_ref, state_ref, ends_ref, pad_ref):
    channels, length = x_ref.shape
    pad_ref[0:8, :] = dot(same((8, length), length - 8).astype(BF16), prev_ref[...], NT)
    pad_ref[8 : 8 + length, :] = dot(same((length, length)).astype(BF16), x_ref[...], NT)
    taps = tap_ref[...].astype(F32)
    conv = jnp.zeros((length, channels), F32)
    for j in range(CONV):
        at = 8 - (CONV - 1) + j
        conv = conv + pad_ref[at : at + length, :] * taps[j : j + 1]
    half = conv.astype(BF16)
    recur = jax.nn.sigmoid(dot(half, carry_ref[0]))
    entry = jax.nn.sigmoid(dot(half, entry_ref[0]))
    fade = jnp.exp(-lane_ref[...])
    series = fade * (1.0 - fade * (0.5 - fade * (1.0 / 3 - fade * (0.25 - fade * 0.2))))
    soft = jnp.where(fade < 0.03, series, jnp.log(1.0 + fade))
    jump = jnp.sum(same((length, length)) * jump_ref[...], axis=1, keepdims=True)
    log_decay = -8.0 * recur * soft + jump
    state = jnp.sqrt(one_minus_exp(2.0 * log_decay)) * entry * conv
    decay = jnp.exp(log_decay)
    rows = lax.broadcasted_iota(jnp.int32, (length, channels), 0)
    step = 1
    while step < length:
        ready = rows >= step
        before_state = jnp.where(ready, pltpu.roll(state, step, 0), 0.0)
        before_decay = jnp.where(ready, pltpu.roll(decay, step, 0), 1.0)
        state = decay * before_state + state
        decay = decay * before_decay
        step *= 2
    decay_ref[...] = decay
    state_ref[...] = state
    ends_ref[...] = jnp.zeros((8, 128), F32)
    for k, value in enumerate((decay[length - 1 : length], state[length - 1 : length])):
        high = value.astype(BF16).astype(F32)
        for j, term in enumerate((high, value - high)):
            r = 2 * k + j
            ends_ref[r : r + 1, :] = term[:, 0:128]
            ends_ref[r + 4 : r + 5, 0 : channels - 128] = term[:, 128:channels]


def local_scan(x, prev, taps, carry, entry, lane, jump):
    channels, length = x.shape
    full = jax.ShapeDtypeStruct((length, channels), F32)
    return pl.pallas_call(
        local_kernel,
        out_shape=(full, full, jax.ShapeDtypeStruct((8, 128), F32)),
        in_specs=[vmem()] * 7,
        out_specs=(vmem(), vmem(), vmem()),
        scratch_shapes=[pltpu.VMEM((length + 8, channels), F32)],
        cost_estimate=cost(100 * length * channels, 16 * length * channels),
        compiler_params=grant(6),
        name="local_scan",
    )(x, prev, taps, carry, entry, lane, jump)


def here(axis):
    return lax.axis_index(axis).astype(jnp.int32).reshape(1)


def on_device(x, valve, taps, carry, entry, lane, jump, tok, scale, routes, scores, expand, contract):
    ep = lax.axis_size("ep")
    width = tok.shape[1] // lax.axis_size("tp")
    at = (here("tp"), here("ep"))
    sent = dispatch(tok, scale[None, :], routes.T, at[0], ep, width)
    arrived = lax.all_to_all(sent.reshape(ep, CAPACITY, width), "ep", 0, 0, tiled=True)
    arrived, flipped = lax.optimization_barrier((arrived, x.T))
    prev = lax.ppermute(flipped, "ep", [(i, i + 1) for i in range(ep - 1)])
    kept = {}

    def hold_prev(block):
        block, kept["prev"] = lax.optimization_barrier((block, prev))
        return block

    def hold_scan(block):
        local = local_scan(flipped, kept["prev"], taps, carry, entry, lane[None, :], jump[None, :])
        block, kept["local"] = lax.optimization_barrier((block, local))
        return block

    half = ep * CAPACITY // 2
    blocks = arrived.reshape(2, half, width)
    hidden = up(blocks, expand[0].T, at, {1: hold_prev, 2: hold_scan})
    decay, state, ends = kept["local"]
    done = down(hidden.reshape(2, half // 2, -1), contract[0], at, ends)
    returned = lax.all_to_all(done, "ep", 0, 0, tiled=True)
    moe, mixed = finish(returned, routes, scores, decay, state, valve.T, at[1])
    return (mixed.T, moe)


def solution(mesh):
    rows = P(("grp", "ep"), None)
    split = P(("grp", "ep"), "tp")
    placed = (
        split,
        split,
        P(None, "tp"),
        P("tp", None, None),
        P("tp", None, None),
        P("tp"),
        P(("grp", "ep")),
        rows,
        P(),
        rows,
        rows,
        P("ep", None, "tp"),
        P("ep", None, "tp"),
    )
    return jax.shard_map(
        on_device, mesh=mesh, in_specs=placed, out_specs=(split, split), check_vma=False
    )
```

```python
import functools

import jax
import jax.numpy as jnp
from jax import lax
from jax.experimental import pallas as pl
from jax.experimental.pallas import tpu as pltpu
from jax.sharding import PartitionSpec as P

CONV = 4
CAPACITY = 24
F32 = jnp.float32
BF16 = jnp.bfloat16

NN = (((1,), (0,)), ((), ()))
NT = (((1,), (1,)), ((), ()))


def dot(a, b, dims=NN):
    return lax.dot_general(a, b, dims, preferred_element_type=F32)


def vmem():
    return pl.BlockSpec(memory_space=pltpu.VMEM)


def smem():
    return pl.BlockSpec(memory_space=pltpu.SMEM)


def cost(flops, nbytes):
    return pl.CostEstimate(flops=flops, bytes_accessed=nbytes, transcendentals=0)


def grant(mebibytes):
    return pltpu.CompilerParams(vmem_limit_bytes=mebibytes * 2**20)


def same(shape, offset=0):
    rows = lax.broadcasted_iota(jnp.int32, shape, 0)
    return (rows + offset == lax.broadcasted_iota(jnp.int32, shape, 1)).astype(F32)


def dispatch_kernel(at_ref, tok_ref, scale_ref, routes_ref, out_ref):
    tokens, features = tok_ref.shape
    slots, width = out_ref.shape
    experts = slots // CAPACITY
    first = pl.multiple_of(at_ref[0] * width, width)
    rows = tok_ref[...].astype(F32)
    mean = jnp.sum(rows, axis=1, keepdims=True) * (1.0 / features)
    centered = rows - mean
    var = jnp.sum(centered * centered, axis=1, keepdims=True) * (1.0 / features)
    part = tok_ref[:, pl.ds(first, width)].astype(F32) - mean
    normed = (part * lax.rsqrt(var + 1e-05) * scale_ref[:, pl.ds(first, width)]).astype(BF16)
    ranks = lax.broadcasted_iota(jnp.int32, (experts, tokens), 0)
    named = [(routes_ref[k : k + 1, :] == ranks).astype(F32) for k in range(2)]
    earlier = (
        lax.broadcasted_iota(jnp.int32, (tokens, tokens), 0)
        < lax.broadcasted_iota(jnp.int32, (tokens, tokens), 1)
    ).astype(F32).astype(BF16)
    place = ranks.astype(F32) * CAPACITY + dot((named[0] + named[1]).astype(BF16), earlier)
    slot = [jnp.sum(m * place, axis=0, keepdims=True).astype(jnp.int32) for m in named]
    ids = lax.broadcasted_iota(jnp.int32, (slots, tokens), 0)
    pick = jnp.logical_or(ids == slot[0], ids == slot[1]).astype(F32).astype(BF16)
    out_ref[...] = dot(pick, normed).astype(BF16)


def dispatch(tok, scale, routes, at, experts, width):
    slots = experts * CAPACITY
    return pl.pallas_call(
        dispatch_kernel,
        out_shape=jax.ShapeDtypeStruct((slots, width), BF16),
        in_specs=[smem(), vmem(), vmem(), vmem()],
        out_specs=vmem(),
        cost_estimate=cost(2 * slots * tok.shape[0] * width, 2 * tok.size + 2 * slots * width),
        name="dispatch",
    )(at, tok, scale, routes)


def combined(ret_ref, routes_ref, score_ref, rows_ref):
    experts = ret_ref.shape[0]
    slots, width = rows_ref.shape
    tokens = routes_ref.shape[0]
    lanes = width // 2
    for e in range(experts):
        for h in range(2):
            part = ret_ref[e, h * CAPACITY : (h + 1) * CAPACITY, :].astype(F32)
            rows_ref[e * CAPACITY : (e + 1) * CAPACITY, h * lanes : (h + 1) * lanes] = part
    rows = rows_ref[...].astype(BF16)
    ranks = lax.broadcasted_iota(jnp.int32, (tokens, experts), 1)
    hot = [(routes_ref[:, k : k + 1] == ranks).astype(F32) for k in range(2)]
    earlier = (
        lax.broadcasted_iota(jnp.int32, (tokens, tokens), 1)
        < lax.broadcasted_iota(jnp.int32, (tokens, tokens), 0)
    ).astype(F32).astype(BF16)
    place = ranks.astype(F32) * CAPACITY + dot(earlier, (hot[0] + hot[1]).astype(BF16))
    ids = lax.broadcasted_iota(jnp.int32, (tokens, slots), 1)
    picked = []
    for m in hot:
        slot = jnp.sum(m * place, axis=1, keepdims=True).astype(jnp.int32)
        picked.append(dot((ids == slot).astype(F32).astype(BF16), rows))
    weight = jax.nn.sigmoid(score_ref[:, 0:1] - score_ref[:, 1:2])
    return weight * picked[0] + (1.0 - weight) * picked[1]


def finish_kernel(at_ref, ret_ref, routes_ref, score_ref, decay_ref, state_ref, valve_ref, moe_ref, mix_ref, rows_ref):
    moe_ref[...] = combined(ret_ref, routes_ref, score_ref, rows_ref).astype(BF16)
    length, channels = state_ref.shape
    me = at_ref[0]
    entering = jnp.zeros((1, 256), F32)
    for d in range(ret_ref.shape[0]):
        ends = ret_ref[d, 2 * CAPACITY : 2 * CAPACITY + 8, :].astype(F32)
        wide = [
            jnp.concatenate([ends[k : k + 1] + ends[k + 1 : k + 2], ends[k + 4 : k + 5] + ends[k + 5 : k + 6]], axis=1)
            for k in (0, 2)
        ]
        entering = jnp.where(d < me, wide[0] * entering + wide[1], entering)
    state = state_ref[...] + decay_ref[...] * entering[:, 0:channels]
    valve = dot(same((length, length)).astype(BF16), valve_ref[...], NT)
    mixed = (state * jax.nn.gelu(valve, approximate=True)).astype(BF16)
    mix_ref[...] = dot(same((channels, channels)).astype(BF16), mixed, NT).astype(BF16)


def finish(returned, routes, scores, decay, state, valve, at):
    slots = returned.shape[0] * CAPACITY
    width = 2 * returned.shape[2]
    tokens = routes.shape[0]
    return pl.pallas_call(
        finish_kernel,
        out_shape=(
            jax.ShapeDtypeStruct((tokens, width), BF16),
            jax.ShapeDtypeStruct(valve.shape, BF16),
        ),
        in_specs=[smem()] + [vmem()] * 6,
        out_specs=(vmem(), vmem()),
        scratch_shapes=[pltpu.VMEM((slots, width), F32)],
        cost_estimate=cost(4 * slots * tokens * width, 4 * slots * width),
        compiler_params=grant(12),
        name="finish",
    )(at, returned, routes, scores, decay, state, valve)


def mirrored(block, sense):
    ep = lax.axis_size("ep")
    tp = lax.axis_size("tp")
    route = []
    for e in range(ep):
        turn = sense if e % 2 == 0 else -sense
        route += [(e * tp + t, e * tp + (t + turn) % tp) for t in range(tp)]
    return lax.ppermute(block, ("ep", "tp"), route)


def ring(block):
    size = lax.axis_size("tp")
    first = second = block
    pieces = [block]
    for _ in range(size // 2 - 1):
        first = mirrored(first, 1)
        second = mirrored(second, -1)
        pieces += [first, second]
    return pieces, [mirrored(first, 1)]


def plain_ring(block, holds):
    size = lax.axis_size("tp")
    ahead = [(i, (i + 1) % size) for i in range(size)]
    back = [(i, (i - 1) % size) for i in range(size)]
    first = second = block
    pieces = [block]
    for hop in range(size // 2 - 1):
        if hop in holds:
            second = holds[hop](second)
        first = lax.ppermute(first, "tp", ahead)
        second = lax.ppermute(second, "tp", back)
        pieces += [first, second]
    return pieces, [lax.ppermute(first[0], "tp", ahead), lax.ppermute(second[1], "tp", back)]


def steps_of(size):
    steps = [0]
    for s in range(1, size // 2):
        steps += [s, -s]
    return steps + [size // 2]


def owner_of(tp_ref, ep_ref, step, size):
    return lax.rem(tp_ref[0] + size + step * (2 * lax.rem(ep_ref[0], 2) - 1), size)


def up_kernel(steps, size, first, tp_ref, ep_ref, *refs):
    pieces, refs = refs[: len(steps)], refs[len(steps) :]
    total_ref, refs = (None, refs) if first else (refs[0], refs[1:])
    w_ref, out_ref = refs
    width = pieces[0].shape[2]
    units = w_ref.shape[0]
    edge = units % 128
    even = units - edge

    def columns(step):
        owner = owner_of(tp_ref, ep_ref, step, size)
        return w_ref[:, pl.ds(pl.multiple_of(owner * width, width), width)]

    for side in range(2):
        total = None if first else total_ref[side]
        for step, piece in zip(steps, pieces):
            term = dot(piece[side], columns(step), NT)
            total = term if total is None else total + term
        if first:
            out_ref[side] = total
            continue
        hidden = (total * jax.nn.sigmoid(total)).astype(BF16)
        out_ref[:, side * even : (side + 1) * even] = hidden[:, 0:even]
        at = 2 * even + side * edge
        out_ref[:, at : at + edge] = hidden[:, even:units]


def down_kernel(steps, size, first, tp_ref, ep_ref, *refs):
    if first:
        pieces, total_ref, ends_ref = refs[: len(steps)], None, None
        blocks = [[piece.at[part] for piece in pieces] for part in range(2)]
    else:
        total_ref, ends_ref = refs[2:4]
        blocks = [[refs[0]], [refs[1]]]
    w_ref, out_ref = refs[-2:]
    rows, both = blocks[0][0].shape
    units = both // 2
    edge = units % 128
    even = units - edge

    def term(block, step, side):
        owner = lax.rem(tp_ref[0] + size - step, size)
        at = 2 * even + side * edge
        mine = jnp.concatenate(
            [block[:, side * even : (side + 1) * even], block[:, at : at + edge]], axis=1
        )
        return dot(mine, w_ref[pl.ds(pl.multiple_of(owner * units, 64), units), :])

    if not first:
        tail = ends_ref[...].astype(BF16)
        for d in range(out_ref.shape[0]):
            out_ref[d, 2 * CAPACITY : 2 * CAPACITY + 8, :] = tail
    for side in range(2):
        for part in range(2):
            span = slice(part * rows, (part + 1) * rows)
            total = None if first else total_ref[side, span]
            for step, block in zip(steps, blocks[part]):
                value = term(block, step, side)
                total = value if total is None else total + value
            if first:
                out_ref[side, span] = total
                continue
            total = total.astype(BF16)
            lanes = total.shape[1] // 2
            group = rows // CAPACITY
            for j in range(group):
                d = (side * 2 + part) * group + j
                mine = total[j * CAPACITY : (j + 1) * CAPACITY]
                out_ref[d, 0:CAPACITY, :] = mine[:, 0:lanes]
                out_ref[d, CAPACITY : 2 * CAPACITY, :] = mine[:, lanes:]


def stage(body, name, steps, pieces, rest, at, out):
    size = lax.axis_size("tp")
    operands = [*pieces, *rest]
    kernel = functools.partial(body, steps, size, len(rest) == 1)
    macs = len(steps) * pieces[0].size * rest[-1].size // pieces[0].shape[-1] // size
    moved = sum(v.size * v.dtype.itemsize for v in operands)
    return pl.pallas_call(
        kernel,
        out_shape=out,
        in_specs=[smem()] * 2 + [vmem()] * len(operands),
        out_specs=vmem(),
        cost_estimate=cost(2 * macs, moved),
        compiler_params=grant(20),
        name=name,
    )(*at, *operands)


def up(block, w, at):
    _, half, _ = block.shape
    units = w.shape[0]
    middle = jax.ShapeDtypeStruct((2, half, units), F32)
    out = jax.ShapeDtypeStruct((half, 2 * units), BF16)
    pieces, far = ring(block)
    steps = steps_of(lax.axis_size("tp"))
    cut = len(pieces)
    total = stage(up_kernel, "up_near", steps[:cut], pieces[:cut], [w], at, middle)
    return stage(up_kernel, "up_far", steps[cut:], pieces[cut:] + far, [total, w], at, out)


def down(block, w, at, holds, ends):
    _, rows, _ = block.shape
    width = w.shape[1]
    middle = jax.ShapeDtypeStruct((2, 2 * rows, width), F32)
    out = jax.ShapeDtypeStruct((4 * rows // CAPACITY, 2 * CAPACITY + 8, width // 2), BF16)
    pieces, far = plain_ring(block, holds)
    steps = steps_of(lax.axis_size("tp"))
    total = stage(down_kernel, "down_near", steps[:-1], pieces, [w], at, middle)
    return stage(down_kernel, "down_far", steps[-1:], far, [total, ends(), w], at, out)


def one_minus_exp(y):
    small = -y * (1.0 + y * (0.5 + y * (1.0 / 6 + y * (1.0 / 24 + y * (1.0 / 120 + y / 720)))))
    return jnp.where(y > -0.25, small, 1.0 - jnp.exp(y))


def local_kernel(x_ref, prev_ref, tap_ref, carry_ref, entry_ref, lane_ref, jump_ref, decay_ref, state_ref, ends_ref, pad_ref):
    channels, length = x_ref.shape
    pad_ref[0:8, :] = dot(same((8, length), length - 8).astype(BF16), prev_ref[...], NT)
    pad_ref[8 : 8 + length, :] = dot(same((length, length)).astype(BF16), x_ref[...], NT)
    taps = tap_ref[...].astype(F32)
    conv = jnp.zeros((length, channels), F32)
    for j in range(CONV):
        at = 8 - (CONV - 1) + j
        conv = conv + pad_ref[at : at + length, :] * taps[j : j + 1]
    half = conv.astype(BF16)
    recur = jax.nn.sigmoid(dot(half, carry_ref[0]))
    entry = jax.nn.sigmoid(dot(half, entry_ref[0]))
    fade = jnp.exp(-lane_ref[...])
    series = fade * (1.0 - fade * (0.5 - fade * (1.0 / 3 - fade * (0.25 - fade * 0.2))))
    soft = jnp.where(fade < 0.03, series, jnp.log(1.0 + fade))
    jump = jnp.sum(same((length, length)) * jump_ref[...], axis=1, keepdims=True)
    log_decay = -8.0 * recur * soft + jump
    state = jnp.sqrt(one_minus_exp(2.0 * log_decay)) * entry * conv
    decay = jnp.exp(log_decay)
    rows = lax.broadcasted_iota(jnp.int32, (length, channels), 0)
    step = 1
    while step < length:
        ready = rows >= step
        before_state = jnp.where(ready, pltpu.roll(state, step, 0), 0.0)
        before_decay = jnp.where(ready, pltpu.roll(decay, step, 0), 1.0)
        state = decay * before_state + state
        decay = decay * before_decay
        step *= 2
    decay_ref[...] = decay
    state_ref[...] = state
    ends_ref[...] = jnp.zeros((8, 128), F32)
    for k, value in enumerate((decay[length - 1 : length], state[length - 1 : length])):
        high = value.astype(BF16).astype(F32)
        for j, term in enumerate((high, value - high)):
            r = 2 * k + j
            ends_ref[r : r + 1, :] = term[:, 0:128]
            ends_ref[r + 4 : r + 5, 0 : channels - 128] = term[:, 128:channels]


def local_scan(x, prev, taps, carry, entry, lane, jump):
    channels, length = x.shape
    full = jax.ShapeDtypeStruct((length, channels), F32)
    return pl.pallas_call(
        local_kernel,
        out_shape=(full, full, jax.ShapeDtypeStruct((8, 128), F32)),
        in_specs=[vmem()] * 7,
        out_specs=(vmem(), vmem(), vmem()),
        scratch_shapes=[pltpu.VMEM((length + 8, channels), F32)],
        cost_estimate=cost(100 * length * channels, 16 * length * channels),
        compiler_params=grant(6),
        name="local_scan",
    )(x, prev, taps, carry, entry, lane, jump)


def here(axis):
    return lax.axis_index(axis).astype(jnp.int32).reshape(1)


def on_device(x, valve, taps, carry, entry, lane, jump, tok, scale, routes, scores, expand, contract):
    ep = lax.axis_size("ep")
    width = tok.shape[1] // lax.axis_size("tp")
    at = (here("tp"), here("ep"))
    sent = dispatch(tok, scale[None, :], routes.T, at[0], ep, width)
    arrived = lax.all_to_all(sent.reshape(ep, CAPACITY, width), "ep", 0, 0, tiled=True)
    half = ep * CAPACITY // 2
    hidden = up(arrived.reshape(2, half, width), expand[0].T, at)
    hidden, flipped = lax.optimization_barrier((hidden, x.T))
    prev = lax.ppermute(flipped, "ep", [(i, i + 1) for i in range(ep - 1)])
    kept = {}

    def hold_prev(block):
        block, kept["prev"] = lax.optimization_barrier((block, prev))
        return block

    def hold_scan(block):
        local = local_scan(flipped, kept["prev"], taps, carry, entry, lane[None, :], jump[None, :])
        block, kept["local"] = lax.optimization_barrier((block, local))
        return block

    holds = {1: hold_prev, 2: hold_scan}
    blocks = hidden.reshape(2, half // 2, -1)
    done = down(blocks, contract[0], at, holds, lambda: kept["local"][2])
    decay, state, _ = kept["local"]
    returned = lax.all_to_all(done, "ep", 0, 0, tiled=True)
    moe, mixed = finish(returned, routes, scores, decay, state, valve.T, at[1])
    return (mixed.T, moe)


def solution(mesh):
    rows = P(("grp", "ep"), None)
    split = P(("grp", "ep"), "tp")
    placed = (
        split,
        split,
        P(None, "tp"),
        P("tp", None, None),
        P("tp", None, None),
        P("tp"),
        P(("grp", "ep")),
        rows,
        P(),
        rows,
        rows,
        P("ep", None, "tp"),
        P("ep", None, "tp"),
    )
    return jax.shard_map(
        on_device, mesh=mesh, in_specs=placed, out_specs=(split, split), check_vma=False
    )
```

```python
import functools

import jax
import jax.numpy as jnp
from jax import lax
from jax.experimental import pallas as pl
from jax.experimental.pallas import tpu as pltpu
from jax.sharding import PartitionSpec as P

CONV = 4
CAPACITY = 24
F32 = jnp.float32
BF16 = jnp.bfloat16

NN = (((1,), (0,)), ((), ()))
NT = (((1,), (1,)), ((), ()))


def dot(a, b, dims=NN):
    return lax.dot_general(a, b, dims, preferred_element_type=F32)


def vmem():
    return pl.BlockSpec(memory_space=pltpu.VMEM)


def smem():
    return pl.BlockSpec(memory_space=pltpu.SMEM)


def cost(flops, nbytes):
    return pl.CostEstimate(flops=flops, bytes_accessed=nbytes, transcendentals=0)


def grant(mebibytes):
    return pltpu.CompilerParams(vmem_limit_bytes=mebibytes * 2**20)


def same(shape, offset=0):
    rows = lax.broadcasted_iota(jnp.int32, shape, 0)
    return (rows + offset == lax.broadcasted_iota(jnp.int32, shape, 1)).astype(F32)


def dispatch_kernel(at_ref, tok_ref, scale_ref, routes_ref, out_ref):
    tokens, features = tok_ref.shape
    slots, width = out_ref.shape
    experts = slots // CAPACITY
    first = pl.multiple_of(at_ref[0] * width, width)
    rows = tok_ref[...].astype(F32)
    mean = jnp.sum(rows, axis=1, keepdims=True) * (1.0 / features)
    centered = rows - mean
    var = jnp.sum(centered * centered, axis=1, keepdims=True) * (1.0 / features)
    part = tok_ref[:, pl.ds(first, width)].astype(F32) - mean
    normed = (part * lax.rsqrt(var + 1e-05) * scale_ref[:, pl.ds(first, width)]).astype(BF16)
    ranks = lax.broadcasted_iota(jnp.int32, (experts, tokens), 0)
    named = [(routes_ref[k : k + 1, :] == ranks).astype(F32) for k in range(2)]
    earlier = (
        lax.broadcasted_iota(jnp.int32, (tokens, tokens), 0)
        < lax.broadcasted_iota(jnp.int32, (tokens, tokens), 1)
    ).astype(F32).astype(BF16)
    place = ranks.astype(F32) * CAPACITY + dot((named[0] + named[1]).astype(BF16), earlier)
    slot = [jnp.sum(m * place, axis=0, keepdims=True).astype(jnp.int32) for m in named]
    ids = lax.broadcasted_iota(jnp.int32, (slots, tokens), 0)
    pick = jnp.logical_or(ids == slot[0], ids == slot[1]).astype(F32).astype(BF16)
    out_ref[...] = dot(pick, normed).astype(BF16)


def dispatch(tok, scale, routes, at, experts, width):
    slots = experts * CAPACITY
    return pl.pallas_call(
        dispatch_kernel,
        out_shape=jax.ShapeDtypeStruct((slots, width), BF16),
        in_specs=[smem(), vmem(), vmem(), vmem()],
        out_specs=vmem(),
        cost_estimate=cost(2 * slots * tok.shape[0] * width, 2 * tok.size + 2 * slots * width),
        name="dispatch",
    )(at, tok, scale, routes)


def combined(ret_ref, routes_ref, score_ref, rows_ref):
    experts = ret_ref.shape[0]
    slots, width = rows_ref.shape
    tokens = routes_ref.shape[0]
    lanes = width // 2
    for e in range(experts):
        for h in range(2):
            part = ret_ref[e, h * CAPACITY : (h + 1) * CAPACITY, :].astype(F32)
            rows_ref[e * CAPACITY : (e + 1) * CAPACITY, h * lanes : (h + 1) * lanes] = part
    rows = rows_ref[...].astype(BF16)
    ranks = lax.broadcasted_iota(jnp.int32, (tokens, experts), 1)
    hot = [(routes_ref[:, k : k + 1] == ranks).astype(F32) for k in range(2)]
    earlier = (
        lax.broadcasted_iota(jnp.int32, (tokens, tokens), 1)
        < lax.broadcasted_iota(jnp.int32, (tokens, tokens), 0)
    ).astype(F32).astype(BF16)
    place = ranks.astype(F32) * CAPACITY + dot(earlier, (hot[0] + hot[1]).astype(BF16))
    ids = lax.broadcasted_iota(jnp.int32, (tokens, slots), 1)
    picked = []
    for m in hot:
        slot = jnp.sum(m * place, axis=1, keepdims=True).astype(jnp.int32)
        picked.append(dot((ids == slot).astype(F32).astype(BF16), rows))
    weight = jax.nn.sigmoid(score_ref[:, 0:1] - score_ref[:, 1:2])
    return weight * picked[0] + (1.0 - weight) * picked[1]


def finish_kernel(at_ref, ret_ref, routes_ref, score_ref, decay_ref, state_ref, valve_ref, moe_ref, mix_ref, rows_ref):
    moe_ref[...] = combined(ret_ref, routes_ref, score_ref, rows_ref).astype(BF16)
    length, channels = state_ref.shape
    me = at_ref[0]
    entering = jnp.zeros((1, 256), F32)
    for d in range(ret_ref.shape[0]):
        ends = ret_ref[d, 2 * CAPACITY : 2 * CAPACITY + 8, :].astype(F32)
        wide = [
            jnp.concatenate([ends[k : k + 1] + ends[k + 1 : k + 2], ends[k + 4 : k + 5] + ends[k + 5 : k + 6]], axis=1)
            for k in (0, 2)
        ]
        entering = jnp.where(d < me, wide[0] * entering + wide[1], entering)
    state = state_ref[...] + decay_ref[...] * entering[:, 0:channels]
    valve = dot(same((length, length)).astype(BF16), valve_ref[...], NT)
    mixed = (state * jax.nn.gelu(valve, approximate=True)).astype(BF16)
    mix_ref[...] = dot(same((channels, channels)).astype(BF16), mixed, NT).astype(BF16)


def finish(returned, routes, scores, decay, state, valve, at):
    slots = returned.shape[0] * CAPACITY
    width = 2 * returned.shape[2]
    tokens = routes.shape[0]
    return pl.pallas_call(
        finish_kernel,
        out_shape=(
            jax.ShapeDtypeStruct((tokens, width), BF16),
            jax.ShapeDtypeStruct(valve.shape, BF16),
        ),
        in_specs=[smem()] + [vmem()] * 6,
        out_specs=(vmem(), vmem()),
        scratch_shapes=[pltpu.VMEM((slots, width), F32)],
        cost_estimate=cost(4 * slots * tokens * width, 4 * slots * width),
        compiler_params=grant(12),
        name="finish",
    )(at, returned, routes, scores, decay, state, valve)


def ring(block, holds):
    size = lax.axis_size("tp")
    ahead = [(i, (i + 1) % size) for i in range(size)]
    back = [(i, (i - 1) % size) for i in range(size)]
    first = second = block
    pieces = [block]
    for hop in range(size // 2 - 1):
        if hop in holds:
            second = holds[hop](second)
        first = lax.ppermute(first, "tp", ahead)
        second = lax.ppermute(second, "tp", back)
        pieces += [first, second]
    return pieces, [lax.ppermute(first[0], "tp", ahead), lax.ppermute(second[1], "tp", back)]


def steps_of(size):
    steps = [0]
    for s in range(1, size // 2):
        steps += [s, -s]
    return steps + [size // 2]


def up_kernel(steps, size, first, tp_ref, *refs):
    total_ref, refs = (None, refs) if first else (refs[-3], (*refs[:-3], *refs[-2:]))
    w_ref, out_ref = refs[-2:]
    whole = len(steps) if first else len(steps) - 1
    width = w_ref.shape[1] // size
    units = w_ref.shape[0]
    edge = units % 128
    even = units - edge

    def columns(step):
        owner = lax.rem(tp_ref[0] + size - step, size)
        return w_ref[:, pl.ds(pl.multiple_of(owner * width, width), width)]

    for side in range(2):
        total = None if first else total_ref[side]
        for step, piece in zip(steps, refs[:whole]):
            term = dot(piece[side], columns(step), NT)
            total = term if total is None else total + term
        if first:
            out_ref[side] = total
            continue
        total = total + dot(refs[whole + side][...], columns(steps[-1]), NT)
        hidden = (total * jax.nn.sigmoid(total)).astype(BF16)
        out_ref[:, side * even : (side + 1) * even] = hidden[:, 0:even]
        at = 2 * even + side * edge
        out_ref[:, at : at + edge] = hidden[:, even:units]


def down_kernel(steps, size, first, tp_ref, *refs):
    if first:
        pieces, total_ref, ends_ref = refs[: len(steps)], None, None
        blocks = [[piece.at[part] for piece in pieces] for part in range(2)]
    else:
        total_ref, ends_ref = refs[2:4]
        blocks = [[refs[0]], [refs[1]]]
    w_ref, out_ref = refs[-2:]
    rows, both = blocks[0][0].shape
    units = both // 2
    edge = units % 128
    even = units - edge

    def term(block, step, side):
        owner = lax.rem(tp_ref[0] + size - step, size)
        at = 2 * even + side * edge
        mine = jnp.concatenate(
            [block[:, side * even : (side + 1) * even], block[:, at : at + edge]], axis=1
        )
        return dot(mine, w_ref[pl.ds(pl.multiple_of(owner * units, 64), units), :])

    if not first:
        tail = ends_ref[...].astype(BF16)
        for d in range(out_ref.shape[0]):
            out_ref[d, 2 * CAPACITY : 2 * CAPACITY + 8, :] = tail
    for side in range(2):
        for part in range(2):
            span = slice(part * rows, (part + 1) * rows)
            total = None if first else total_ref[side, span]
            for step, block in zip(steps, blocks[part]):
                value = term(block, step, side)
                total = value if total is None else total + value
            if first:
                out_ref[side, span] = total
                continue
            total = total.astype(BF16)
            lanes = total.shape[1] // 2
            group = rows // CAPACITY
            for j in range(group):
                d = (side * 2 + part) * group + j
                mine = total[j * CAPACITY : (j + 1) * CAPACITY]
                out_ref[d, 0:CAPACITY, :] = mine[:, 0:lanes]
                out_ref[d, CAPACITY : 2 * CAPACITY, :] = mine[:, lanes:]


def stage(body, name, steps, pieces, rest, at, out):
    size = lax.axis_size("tp")
    operands = [*pieces, *rest]
    kernel = functools.partial(body, steps, size, len(rest) == 1)
    macs = len(steps) * pieces[0].size * rest[-1].size // pieces[0].shape[-1] // size
    moved = sum(v.size * v.dtype.itemsize for v in operands)
    return pl.pallas_call(
        kernel,
        out_shape=out,
        in_specs=[smem()] + [vmem()] * len(operands),
        out_specs=vmem(),
        cost_estimate=cost(2 * macs, moved),
        compiler_params=grant(20),
        name=name,
    )(at, *operands)


def up(block, w, at):
    _, half, _ = block.shape
    units = w.shape[0]
    middle = jax.ShapeDtypeStruct((2, half, units), F32)
    out = jax.ShapeDtypeStruct((half, 2 * units), BF16)
    pieces, far = ring(block, {})
    steps = steps_of(lax.axis_size("tp"))
    cut = len(pieces) - 2
    total = stage(up_kernel, "up_near", steps[:cut], pieces[:cut], [w], at, middle)
    return stage(up_kernel, "up_far", steps[cut:], pieces[cut:] + far, [total, w], at, out)


def down(block, w, at, holds, ends):
    _, rows, _ = block.shape
    width = w.shape[1]
    middle = jax.ShapeDtypeStruct((2, 2 * rows, width), F32)
    out = jax.ShapeDtypeStruct((4 * rows // CAPACITY, 2 * CAPACITY + 8, width // 2), BF16)
    pieces, far = ring(block, holds)
    steps = steps_of(lax.axis_size("tp"))
    total = stage(down_kernel, "down_near", steps[:-1], pieces, [w], at, middle)
    return stage(down_kernel, "down_far", steps[-1:], far, [total, ends(), w], at, out)


def one_minus_exp(y):
    small = -y * (1.0 + y * (0.5 + y * (1.0 / 6 + y * (1.0 / 24 + y * (1.0 / 120 + y / 720)))))
    return jnp.where(y > -0.25, small, 1.0 - jnp.exp(y))


def local_kernel(x_ref, prev_ref, tap_ref, carry_ref, entry_ref, lane_ref, jump_ref, decay_ref, state_ref, ends_ref, pad_ref):
    channels, length = x_ref.shape
    pad_ref[0:8, :] = dot(same((8, length), length - 8).astype(BF16), prev_ref[...], NT)
    pad_ref[8 : 8 + length, :] = dot(same((length, length)).astype(BF16), x_ref[...], NT)
    taps = tap_ref[...].astype(F32)
    conv = jnp.zeros((length, channels), F32)
    for j in range(CONV):
        at = 8 - (CONV - 1) + j
        conv = conv + pad_ref[at : at + length, :] * taps[j : j + 1]
    half = conv.astype(BF16)
    recur = jax.nn.sigmoid(dot(half, carry_ref[0]))
    entry = jax.nn.sigmoid(dot(half, entry_ref[0]))
    fade = jnp.exp(-lane_ref[...])
    series = fade * (1.0 - fade * (0.5 - fade * (1.0 / 3 - fade * (0.25 - fade * 0.2))))
    soft = jnp.where(fade < 0.03, series, jnp.log(1.0 + fade))
    jump = jnp.sum(same((length, length)) * jump_ref[...], axis=1, keepdims=True)
    log_decay = -8.0 * recur * soft + jump
    state = jnp.sqrt(one_minus_exp(2.0 * log_decay)) * entry * conv
    decay = jnp.exp(log_decay)
    rows = lax.broadcasted_iota(jnp.int32, (length, channels), 0)
    step = 1
    while step < length:
        ready = rows >= step
        before_state = jnp.where(ready, pltpu.roll(state, step, 0), 0.0)
        before_decay = jnp.where(ready, pltpu.roll(decay, step, 0), 1.0)
        state = decay * before_state + state
        decay = decay * before_decay
        step *= 2
    decay_ref[...] = decay
    state_ref[...] = state
    ends_ref[...] = jnp.zeros((8, 128), F32)
    for k, value in enumerate((decay[length - 1 : length], state[length - 1 : length])):
        high = value.astype(BF16).astype(F32)
        for j, term in enumerate((high, value - high)):
            r = 2 * k + j
            ends_ref[r : r + 1, :] = term[:, 0:128]
            ends_ref[r + 4 : r + 5, 0 : channels - 128] = term[:, 128:channels]


def local_scan(x, prev, taps, carry, entry, lane, jump):
    channels, length = x.shape
    full = jax.ShapeDtypeStruct((length, channels), F32)
    return pl.pallas_call(
        local_kernel,
        out_shape=(full, full, jax.ShapeDtypeStruct((8, 128), F32)),
        in_specs=[vmem()] * 7,
        out_specs=(vmem(), vmem(), vmem()),
        scratch_shapes=[pltpu.VMEM((length + 8, channels), F32)],
        cost_estimate=cost(100 * length * channels, 16 * length * channels),
        compiler_params=grant(6),
        name="local_scan",
    )(x, prev, taps, carry, entry, lane, jump)


def here(axis):
    return lax.axis_index(axis).astype(jnp.int32).reshape(1)


def on_device(x, valve, taps, carry, entry, lane, jump, tok, scale, routes, scores, expand, contract):
    ep = lax.axis_size("ep")
    width = tok.shape[1] // lax.axis_size("tp")
    at = here("tp")
    sent = dispatch(tok, scale[None, :], routes.T, at, ep, width)
    arrived = lax.all_to_all(sent.reshape(ep, CAPACITY, width), "ep", 0, 0, tiled=True)
    half = ep * CAPACITY // 2
    hidden = up(arrived.reshape(2, half, width), expand[0].T, at)
    hidden, flipped = lax.optimization_barrier((hidden, x.T))
    prev = lax.ppermute(flipped, "ep", [(i, i + 1) for i in range(ep - 1)])
    kept = {}

    def hold_prev(block):
        block, kept["prev"] = lax.optimization_barrier((block, prev))
        return block

    def hold_scan(block):
        local = local_scan(flipped, kept["prev"], taps, carry, entry, lane[None, :], jump[None, :])
        block, kept["local"] = lax.optimization_barrier((block, local))
        return block

    holds = {1: hold_prev, 2: hold_scan}
    blocks = hidden.reshape(2, half // 2, -1)
    done = down(blocks, contract[0], at, holds, lambda: kept["local"][2])
    decay, state, _ = kept["local"]
    returned = lax.all_to_all(done, "ep", 0, 0, tiled=True)
    moe, mixed = finish(returned, routes, scores, decay, state, valve.T, here("ep"))
    return (mixed.T, moe)


def solution(mesh):
    rows = P(("grp", "ep"), None)
    split = P(("grp", "ep"), "tp")
    placed = (
        split,
        split,
        P(None, "tp"),
        P("tp", None, None),
        P("tp", None, None),
        P("tp"),
        P(("grp", "ep")),
        rows,
        P(),
        rows,
        rows,
        P("ep", None, "tp"),
        P("ep", None, "tp"),
    )
    return jax.shard_map(
        on_device, mesh=mesh, in_specs=placed, out_specs=(split, split), check_vma=False
    )
```

```python
import functools

import jax
import jax.numpy as jnp
from jax import lax
from jax.experimental import pallas as pl
from jax.experimental.pallas import tpu as pltpu
from jax.sharding import PartitionSpec as P

CONV = 4
CAPACITY = 24
F32 = jnp.float32
BF16 = jnp.bfloat16

NN = (((1,), (0,)), ((), ()))
NT = (((1,), (1,)), ((), ()))


def dot(a, b, dims=NN):
    return lax.dot_general(a, b, dims, preferred_element_type=F32)


def vmem():
    return pl.BlockSpec(memory_space=pltpu.VMEM)


def smem():
    return pl.BlockSpec(memory_space=pltpu.SMEM)


def cost(flops, nbytes):
    return pl.CostEstimate(flops=flops, bytes_accessed=nbytes, transcendentals=0)


def grant(mebibytes):
    return pltpu.CompilerParams(vmem_limit_bytes=mebibytes * 2**20)


def same(shape, offset=0):
    rows = lax.broadcasted_iota(jnp.int32, shape, 0)
    return (rows + offset == lax.broadcasted_iota(jnp.int32, shape, 1)).astype(F32)


def dispatch_kernel(at_ref, tok_ref, scale_ref, routes_ref, out_ref):
    tokens, features = tok_ref.shape
    slots, width = out_ref.shape
    experts = slots // CAPACITY
    first = pl.multiple_of(at_ref[0] * width, width)
    rows = tok_ref[...].astype(F32)
    mean = jnp.sum(rows, axis=1, keepdims=True) * (1.0 / features)
    centered = rows - mean
    var = jnp.sum(centered * centered, axis=1, keepdims=True) * (1.0 / features)
    part = tok_ref[:, pl.ds(first, width)].astype(F32) - mean
    normed = (part * lax.rsqrt(var + 1e-05) * scale_ref[:, pl.ds(first, width)]).astype(BF16)
    ranks = lax.broadcasted_iota(jnp.int32, (experts, tokens), 0)
    named = [(routes_ref[k : k + 1, :] == ranks).astype(F32) for k in range(2)]
    earlier = (
        lax.broadcasted_iota(jnp.int32, (tokens, tokens), 0)
        < lax.broadcasted_iota(jnp.int32, (tokens, tokens), 1)
    ).astype(F32).astype(BF16)
    place = ranks.astype(F32) * CAPACITY + dot((named[0] + named[1]).astype(BF16), earlier)
    slot = [jnp.sum(m * place, axis=0, keepdims=True).astype(jnp.int32) for m in named]
    ids = lax.broadcasted_iota(jnp.int32, (slots, tokens), 0)
    pick = jnp.logical_or(ids == slot[0], ids == slot[1]).astype(F32).astype(BF16)
    out_ref[...] = dot(pick, normed).astype(BF16)


def dispatch(tok, scale, routes, at, experts, width):
    slots = experts * CAPACITY
    return pl.pallas_call(
        dispatch_kernel,
        out_shape=jax.ShapeDtypeStruct((slots, width), BF16),
        in_specs=[smem(), vmem(), vmem(), vmem()],
        out_specs=vmem(),
        cost_estimate=cost(2 * slots * tok.shape[0] * width, 2 * tok.size + 2 * slots * width),
        name="dispatch",
    )(at, tok, scale, routes)


def combined(ret_ref, routes_ref, score_ref, rows_ref):
    experts = ret_ref.shape[0]
    slots, width = rows_ref.shape
    tokens = routes_ref.shape[0]
    lanes = width // 2
    for e in range(experts):
        for h in range(2):
            part = ret_ref[e, h * CAPACITY : (h + 1) * CAPACITY, :].astype(F32)
            rows_ref[e * CAPACITY : (e + 1) * CAPACITY, h * lanes : (h + 1) * lanes] = part
    rows = rows_ref[...].astype(BF16)
    ranks = lax.broadcasted_iota(jnp.int32, (tokens, experts), 1)
    hot = [(routes_ref[:, k : k + 1] == ranks).astype(F32) for k in range(2)]
    earlier = (
        lax.broadcasted_iota(jnp.int32, (tokens, tokens), 1)
        < lax.broadcasted_iota(jnp.int32, (tokens, tokens), 0)
    ).astype(F32).astype(BF16)
    place = ranks.astype(F32) * CAPACITY + dot(earlier, (hot[0] + hot[1]).astype(BF16))
    ids = lax.broadcasted_iota(jnp.int32, (tokens, slots), 1)
    picked = []
    for m in hot:
        slot = jnp.sum(m * place, axis=1, keepdims=True).astype(jnp.int32)
        picked.append(dot((ids == slot).astype(F32).astype(BF16), rows))
    weight = jax.nn.sigmoid(score_ref[:, 0:1] - score_ref[:, 1:2])
    return weight * picked[0] + (1.0 - weight) * picked[1]


def finish_kernel(at_ref, ret_ref, routes_ref, score_ref, decay_ref, state_ref, valve_ref, moe_ref, mix_ref, rows_ref):
    moe_ref[...] = combined(ret_ref, routes_ref, score_ref, rows_ref).astype(BF16)
    length, channels = state_ref.shape
    me = at_ref[0]
    entering = jnp.zeros((1, 256), F32)
    for d in range(ret_ref.shape[0]):
        ends = ret_ref[d, 2 * CAPACITY : 2 * CAPACITY + 8, :].astype(F32)
        wide = [
            jnp.concatenate([ends[k : k + 1] + ends[k + 1 : k + 2], ends[k + 4 : k + 5] + ends[k + 5 : k + 6]], axis=1)
            for k in (0, 2)
        ]
        entering = jnp.where(d < me, wide[0] * entering + wide[1], entering)
    state = state_ref[...] + decay_ref[...] * entering[:, 0:channels]
    valve = dot(same((length, length)).astype(BF16), valve_ref[...], NT)
    mixed = (state * jax.nn.gelu(valve, approximate=True)).astype(BF16)
    mix_ref[...] = dot(same((channels, channels)).astype(BF16), mixed, NT).astype(BF16)


def finish(returned, routes, scores, decay, state, valve, at):
    slots = returned.shape[0] * CAPACITY
    width = 2 * returned.shape[2]
    tokens = routes.shape[0]
    return pl.pallas_call(
        finish_kernel,
        out_shape=(
            jax.ShapeDtypeStruct((tokens, width), BF16),
            jax.ShapeDtypeStruct(valve.shape, BF16),
        ),
        in_specs=[smem()] + [vmem()] * 6,
        out_specs=(vmem(), vmem()),
        scratch_shapes=[pltpu.VMEM((slots, width), F32)],
        cost_estimate=cost(4 * slots * tokens * width, 4 * slots * width),
        compiler_params=grant(12),
        name="finish",
    )(at, returned, routes, scores, decay, state, valve)


def ring(block, holds):
    size = lax.axis_size("tp")
    ahead = [(i, (i + 1) % size) for i in range(size)]
    back = [(i, (i - 1) % size) for i in range(size)]
    first = second = block
    pieces = [block]
    for hop in range(size // 2 - 1):
        if hop in holds:
            first = holds[hop](first)
        first = lax.ppermute(first, "tp", ahead)
        second = lax.ppermute(second, "tp", back)
        pieces += [first, second]
    return pieces, [lax.ppermute(first[0], "tp", ahead), lax.ppermute(second[1], "tp", back)]


def steps_of(size):
    steps = [0]
    for s in range(1, size // 2):
        steps += [s, -s]
    return steps + [size // 2]


def up_kernel(steps, size, first, tp_ref, *refs):
    total_ref, refs = (None, refs) if first else (refs[-3], (*refs[:-3], *refs[-2:]))
    w_ref, out_ref = refs[-2:]
    whole = len(steps) if first else len(steps) - 1
    width = w_ref.shape[1] // size
    units = w_ref.shape[0]
    edge = units % 128
    even = units - edge

    def columns(step):
        owner = lax.rem(tp_ref[0] + size - step, size)
        return w_ref[:, pl.ds(pl.multiple_of(owner * width, width), width)]

    for side in range(2):
        total = None if first else total_ref[side]
        for step, piece in zip(steps, refs[:whole]):
            term = dot(piece[side], columns(step), NT)
            total = term if total is None else total + term
        if first:
            out_ref[side] = total
            continue
        total = total + dot(refs[whole + side][...], columns(steps[-1]), NT)
        hidden = (total * jax.nn.sigmoid(total)).astype(BF16)
        out_ref[:, side * even : (side + 1) * even] = hidden[:, 0:even]
        at = 2 * even + side * edge
        out_ref[:, at : at + edge] = hidden[:, even:units]


def down_kernel(steps, size, first, tp_ref, *refs):
    if first:
        pieces, total_ref, ends_ref = refs[: len(steps)], None, None
        blocks = [[piece.at[part] for piece in pieces] for part in range(2)]
    else:
        total_ref, ends_ref = refs[2:4]
        blocks = [[refs[0]], [refs[1]]]
    w_ref, out_ref = refs[-2:]
    rows, both = blocks[0][0].shape
    units = both // 2
    edge = units % 128
    even = units - edge

    def term(block, step, side):
        owner = lax.rem(tp_ref[0] + size - step, size)
        at = 2 * even + side * edge
        mine = jnp.concatenate(
            [block[:, side * even : (side + 1) * even], block[:, at : at + edge]], axis=1
        )
        return dot(mine, w_ref[pl.ds(pl.multiple_of(owner * units, 64), units), :])

    if not first:
        tail = ends_ref[...].astype(BF16)
        for d in range(out_ref.shape[0]):
            out_ref[d, 2 * CAPACITY : 2 * CAPACITY + 8, :] = tail
    for side in range(2):
        for part in range(2):
            span = slice(part * rows, (part + 1) * rows)
            total = None if first else total_ref[side, span]
            for step, block in zip(steps, blocks[part]):
                value = term(block, step, side)
                total = value if total is None else total + value
            if first:
                out_ref[side, span] = total
                continue
            total = total.astype(BF16)
            lanes = total.shape[1] // 2
            group = rows // CAPACITY
            for j in range(group):
                d = (side * 2 + part) * group + j
                mine = total[j * CAPACITY : (j + 1) * CAPACITY]
                out_ref[d, 0:CAPACITY, :] = mine[:, 0:lanes]
                out_ref[d, CAPACITY : 2 * CAPACITY, :] = mine[:, lanes:]


def stage(body, name, steps, pieces, rest, at, out):
    size = lax.axis_size("tp")
    operands = [*pieces, *rest]
    kernel = functools.partial(body, steps, size, len(rest) == 1)
    macs = len(steps) * pieces[0].size * rest[-1].size // pieces[0].shape[-1] // size
    moved = sum(v.size * v.dtype.itemsize for v in operands)
    return pl.pallas_call(
        kernel,
        out_shape=out,
        in_specs=[smem()] + [vmem()] * len(operands),
        out_specs=vmem(),
        cost_estimate=cost(2 * macs, moved),
        compiler_params=grant(20),
        name=name,
    )(at, *operands)


def up(block, w, at):
    _, half, _ = block.shape
    units = w.shape[0]
    middle = jax.ShapeDtypeStruct((2, half, units), F32)
    out = jax.ShapeDtypeStruct((half, 2 * units), BF16)
    pieces, far = ring(block, {})
    steps = steps_of(lax.axis_size("tp"))
    cut = len(pieces) - 2
    total = stage(up_kernel, "up_near", steps[:cut], pieces[:cut], [w], at, middle)
    return stage(up_kernel, "up_far", steps[cut:], pieces[cut:] + far, [total, w], at, out)


def down(block, w, at, holds, ends):
    _, rows, _ = block.shape
    width = w.shape[1]
    middle = jax.ShapeDtypeStruct((2, 2 * rows, width), F32)
    out = jax.ShapeDtypeStruct((4 * rows // CAPACITY, 2 * CAPACITY + 8, width // 2), BF16)
    pieces, far = ring(block, holds)
    steps = steps_of(lax.axis_size("tp"))
    total = stage(down_kernel, "down_near", steps[:-1], pieces, [w], at, middle)
    return stage(down_kernel, "down_far", steps[-1:], far, [total, ends(), w], at, out)


def one_minus_exp(y):
    small = -y * (1.0 + y * (0.5 + y * (1.0 / 6 + y * (1.0 / 24 + y * (1.0 / 120 + y / 720)))))
    return jnp.where(y > -0.25, small, 1.0 - jnp.exp(y))


def local_kernel(x_ref, prev_ref, tap_ref, carry_ref, entry_ref, lane_ref, jump_ref, decay_ref, state_ref, ends_ref, pad_ref):
    channels, length = x_ref.shape
    pad_ref[0:8, :] = dot(same((8, length), length - 8).astype(BF16), prev_ref[...], NT)
    pad_ref[8 : 8 + length, :] = dot(same((length, length)).astype(BF16), x_ref[...], NT)
    taps = tap_ref[...].astype(F32)
    conv = jnp.zeros((length, channels), F32)
    for j in range(CONV):
        at = 8 - (CONV - 1) + j
        conv = conv + pad_ref[at : at + length, :] * taps[j : j + 1]
    half = conv.astype(BF16)
    recur = jax.nn.sigmoid(dot(half, carry_ref[0]))
    entry = jax.nn.sigmoid(dot(half, entry_ref[0]))
    fade = jnp.exp(-lane_ref[...])
    series = fade * (1.0 - fade * (0.5 - fade * (1.0 / 3 - fade * (0.25 - fade * 0.2))))
    soft = jnp.where(fade < 0.03, series, jnp.log(1.0 + fade))
    jump = jnp.sum(same((length, length)) * jump_ref[...], axis=1, keepdims=True)
    log_decay = -8.0 * recur * soft + jump
    state = jnp.sqrt(one_minus_exp(2.0 * log_decay)) * entry * conv
    decay = jnp.exp(log_decay)
    rows = lax.broadcasted_iota(jnp.int32, (length, channels), 0)
    step = 1
    while step < length:
        ready = rows >= step
        before_state = jnp.where(ready, pltpu.roll(state, step, 0), 0.0)
        before_decay = jnp.where(ready, pltpu.roll(decay, step, 0), 1.0)
        state = decay * before_state + state
        decay = decay * before_decay
        step *= 2
    decay_ref[...] = decay
    state_ref[...] = state
    ends_ref[...] = jnp.zeros((8, 128), F32)
    for k, value in enumerate((decay[length - 1 : length], state[length - 1 : length])):
        high = value.astype(BF16).astype(F32)
        for j, term in enumerate((high, value - high)):
            r = 2 * k + j
            ends_ref[r : r + 1, :] = term[:, 0:128]
            ends_ref[r + 4 : r + 5, 0 : channels - 128] = term[:, 128:channels]


def local_scan(x, prev, taps, carry, entry, lane, jump):
    channels, length = x.shape
    full = jax.ShapeDtypeStruct((length, channels), F32)
    return pl.pallas_call(
        local_kernel,
        out_shape=(full, full, jax.ShapeDtypeStruct((8, 128), F32)),
        in_specs=[vmem()] * 7,
        out_specs=(vmem(), vmem(), vmem()),
        scratch_shapes=[pltpu.VMEM((length + 8, channels), F32)],
        cost_estimate=cost(100 * length * channels, 16 * length * channels),
        compiler_params=grant(6),
        name="local_scan",
    )(x, prev, taps, carry, entry, lane, jump)


def here(axis):
    return lax.axis_index(axis).astype(jnp.int32).reshape(1)


def on_device(x, valve, taps, carry, entry, lane, jump, tok, scale, routes, scores, expand, contract):
    ep = lax.axis_size("ep")
    width = tok.shape[1] // lax.axis_size("tp")
    at = here("tp")
    sent = dispatch(tok, scale[None, :], routes.T, at, ep, width)
    arrived = lax.all_to_all(sent.reshape(ep, CAPACITY, width), "ep", 0, 0, tiled=True)
    half = ep * CAPACITY // 2
    hidden = up(arrived.reshape(2, half, width), expand[0].T, at)
    hidden, flipped = lax.optimization_barrier((hidden, x.T))
    prev = lax.ppermute(flipped, "ep", [(i, i + 1) for i in range(ep - 1)])
    kept = {}

    def hold_prev(block):
        block, kept["prev"] = lax.optimization_barrier((block, prev))
        return block

    def hold_scan(block):
        local = local_scan(flipped, kept["prev"], taps, carry, entry, lane[None, :], jump[None, :])
        block, kept["local"] = lax.optimization_barrier((block, local))
        return block

    holds = {1: hold_prev, 2: hold_scan}
    blocks = hidden.reshape(2, half // 2, -1)
    done = down(blocks, contract[0], at, holds, lambda: kept["local"][2])
    decay, state, _ = kept["local"]
    returned = lax.all_to_all(done, "ep", 0, 0, tiled=True)
    moe, mixed = finish(returned, routes, scores, decay, state, valve.T, here("ep"))
    return (mixed.T, moe)


def solution(mesh):
    rows = P(("grp", "ep"), None)
    split = P(("grp", "ep"), "tp")
    placed = (
        split,
        split,
        P(None, "tp"),
        P("tp", None, None),
        P("tp", None, None),
        P("tp"),
        P(("grp", "ep")),
        rows,
        P(),
        rows,
        rows,
        P("ep", None, "tp"),
        P("ep", None, "tp"),
    )
    return jax.shard_map(
        on_device, mesh=mesh, in_specs=placed, out_specs=(split, split), check_vma=False
    )
```

```python
import functools

import jax
import jax.numpy as jnp
from jax import lax
from jax.experimental import pallas as pl
from jax.experimental.pallas import tpu as pltpu
from jax.sharding import PartitionSpec as P

CONV = 4
CAPACITY = 24
F32 = jnp.float32
BF16 = jnp.bfloat16

NN = (((1,), (0,)), ((), ()))
NT = (((1,), (1,)), ((), ()))


def dot(a, b, dims=NN):
    return lax.dot_general(a, b, dims, preferred_element_type=F32)


def vmem():
    return pl.BlockSpec(memory_space=pltpu.VMEM)


def smem():
    return pl.BlockSpec(memory_space=pltpu.SMEM)


def cost(flops, nbytes):
    return pl.CostEstimate(flops=flops, bytes_accessed=nbytes, transcendentals=0)


def grant(mebibytes):
    return pltpu.CompilerParams(vmem_limit_bytes=mebibytes * 2**20)


def same(shape, offset=0):
    rows = lax.broadcasted_iota(jnp.int32, shape, 0)
    return (rows + offset == lax.broadcasted_iota(jnp.int32, shape, 1)).astype(F32)


PARTS = 4


def dispatch_kernel(at_ref, tok_hbm, scale_hbm, routes_hbm, out_ref, tok_ref, scale_ref, routes_ref, normed_ref, sems):
    tokens, features = tok_ref.shape
    slots, width = out_ref.shape
    experts = slots // CAPACITY
    rows = tokens // PARTS
    first = pl.multiple_of(at_ref[0] * width, width)
    routes_copy = pltpu.make_async_copy(routes_hbm, routes_ref, sems.at[0])
    scale_copy = pltpu.make_async_copy(scale_hbm.at[:, pl.ds(first, width)], scale_ref, sems.at[1])
    tok_copies = [
        pltpu.make_async_copy(
            tok_hbm.at[pl.ds(c * rows, rows)], tok_ref.at[pl.ds(c * rows, rows)], sems.at[2 + c]
        )
        for c in range(PARTS)
    ]
    for copy in (routes_copy, *tok_copies, scale_copy):
        copy.start()
    routes_copy.wait()
    ranks = lax.broadcasted_iota(jnp.int32, (experts, tokens), 0)
    named = [(routes_ref[k : k + 1, :] == ranks).astype(F32) for k in range(2)]
    earlier = (
        lax.broadcasted_iota(jnp.int32, (tokens, tokens), 0)
        < lax.broadcasted_iota(jnp.int32, (tokens, tokens), 1)
    ).astype(F32).astype(BF16)
    place = ranks.astype(F32) * CAPACITY + dot((named[0] + named[1]).astype(BF16), earlier)
    slot = [jnp.sum(m * place, axis=0, keepdims=True).astype(jnp.int32) for m in named]
    ids = lax.broadcasted_iota(jnp.int32, (slots, tokens), 0)
    pick = jnp.logical_or(ids == slot[0], ids == slot[1]).astype(F32).astype(BF16)
    scale_copy.wait()
    for c in range(PARTS):
        tok_copies[c].wait()
        part = tok_ref[c * rows : (c + 1) * rows, :].astype(F32)
        mean = jnp.sum(part, axis=1, keepdims=True) * (1.0 / features)
        centered = part - mean
        var = jnp.sum(centered * centered, axis=1, keepdims=True) * (1.0 / features)
        mine = tok_ref[c * rows : (c + 1) * rows, pl.ds(first, width)].astype(F32) - mean
        normed = mine * lax.rsqrt(var + 1e-05) * scale_ref[...]
        normed_ref[c * rows : (c + 1) * rows, :] = normed.astype(BF16)
    out_ref[...] = dot(pick, normed_ref[...]).astype(BF16)


def dispatch(tok, scale, routes, at, experts, width):
    slots = experts * CAPACITY
    tokens = tok.shape[0]
    far = pl.BlockSpec(memory_space=pltpu.HBM)
    return pl.pallas_call(
        dispatch_kernel,
        out_shape=jax.ShapeDtypeStruct((slots, width), BF16),
        in_specs=[smem(), far, far, far],
        out_specs=vmem(),
        scratch_shapes=[
            pltpu.VMEM(tok.shape, BF16),
            pltpu.VMEM((1, width), F32),
            pltpu.VMEM(routes.shape, jnp.int32),
            pltpu.VMEM((tokens, width), BF16),
            pltpu.SemaphoreType.DMA((2 + PARTS,)),
        ],
        cost_estimate=cost(2 * slots * tokens * width, 2 * tok.size + 2 * slots * width),
        name="dispatch",
    )(at, tok, scale, routes)


def combined(ret_ref, routes_ref, score_ref, rows_ref):
    experts = ret_ref.shape[0]
    slots, width = rows_ref.shape
    tokens = routes_ref.shape[0]
    lanes = width // 2
    for e in range(experts):
        for h in range(2):
            part = ret_ref[e, h * CAPACITY : (h + 1) * CAPACITY, :].astype(F32)
            rows_ref[e * CAPACITY : (e + 1) * CAPACITY, h * lanes : (h + 1) * lanes] = part
    rows = rows_ref[...].astype(BF16)
    ranks = lax.broadcasted_iota(jnp.int32, (tokens, experts), 1)
    hot = [(routes_ref[:, k : k + 1] == ranks).astype(F32) for k in range(2)]
    earlier = (
        lax.broadcasted_iota(jnp.int32, (tokens, tokens), 1)
        < lax.broadcasted_iota(jnp.int32, (tokens, tokens), 0)
    ).astype(F32).astype(BF16)
    place = ranks.astype(F32) * CAPACITY + dot(earlier, (hot[0] + hot[1]).astype(BF16))
    ids = lax.broadcasted_iota(jnp.int32, (tokens, slots), 1)
    picked = []
    for m in hot:
        slot = jnp.sum(m * place, axis=1, keepdims=True).astype(jnp.int32)
        picked.append(dot((ids == slot).astype(F32).astype(BF16), rows))
    weight = jax.nn.sigmoid(score_ref[:, 0:1] - score_ref[:, 1:2])
    return weight * picked[0] + (1.0 - weight) * picked[1]


def finish_kernel(at_ref, ret_ref, routes_ref, score_ref, decay_ref, state_ref, valve_ref, moe_ref, mix_ref, rows_ref):
    moe_ref[...] = combined(ret_ref, routes_ref, score_ref, rows_ref).astype(BF16)
    length, channels = state_ref.shape
    me = at_ref[0]
    entering = jnp.zeros((1, 256), F32)
    for d in range(ret_ref.shape[0]):
        ends = ret_ref[d, 2 * CAPACITY : 2 * CAPACITY + 8, :].astype(F32)
        wide = [
            jnp.concatenate([ends[k : k + 1] + ends[k + 1 : k + 2], ends[k + 4 : k + 5] + ends[k + 5 : k + 6]], axis=1)
            for k in (0, 2)
        ]
        entering = jnp.where(d < me, wide[0] * entering + wide[1], entering)
    state = state_ref[...] + decay_ref[...] * entering[:, 0:channels]
    valve = dot(same((length, length)).astype(BF16), valve_ref[...], NT)
    mixed = (state * jax.nn.gelu(valve, approximate=True)).astype(BF16)
    mix_ref[...] = dot(same((channels, channels)).astype(BF16), mixed, NT).astype(BF16)


def finish(returned, routes, scores, decay, state, valve, at):
    slots = returned.shape[0] * CAPACITY
    width = 2 * returned.shape[2]
    tokens = routes.shape[0]
    return pl.pallas_call(
        finish_kernel,
        out_shape=(
            jax.ShapeDtypeStruct((tokens, width), BF16),
            jax.ShapeDtypeStruct(valve.shape, BF16),
        ),
        in_specs=[smem()] + [vmem()] * 6,
        out_specs=(vmem(), vmem()),
        scratch_shapes=[pltpu.VMEM((slots, width), F32)],
        cost_estimate=cost(4 * slots * tokens * width, 4 * slots * width),
        compiler_params=grant(12),
        name="finish",
    )(at, returned, routes, scores, decay, state, valve)


def ring(block, holds):
    size = lax.axis_size("tp")
    ahead = [(i, (i + 1) % size) for i in range(size)]
    back = [(i, (i - 1) % size) for i in range(size)]
    first = second = block
    pieces = [block]
    for hop in range(size // 2 - 1):
        if hop in holds:
            first = holds[hop](first)
        first = lax.ppermute(first, "tp", ahead)
        second = lax.ppermute(second, "tp", back)
        pieces += [first, second]
    return pieces, [lax.ppermute(first[0], "tp", ahead), lax.ppermute(second[1], "tp", back)]


def steps_of(size):
    steps = [0]
    for s in range(1, size // 2):
        steps += [s, -s]
    return steps + [size // 2]


def up_kernel(steps, size, first, tp_ref, *refs):
    total_ref, refs = (None, refs) if first else (refs[-3], (*refs[:-3], *refs[-2:]))
    w_ref, out_ref = refs[-2:]
    whole = len(steps) if first else len(steps) - 1
    width = w_ref.shape[1] // size
    units = w_ref.shape[0]
    edge = units % 128
    even = units - edge

    def columns(step):
        owner = lax.rem(tp_ref[0] + size - step, size)
        return w_ref[:, pl.ds(pl.multiple_of(owner * width, width), width)]

    for side in range(2):
        total = None if first else total_ref[side]
        for step, piece in zip(steps, refs[:whole]):
            term = dot(piece[side], columns(step), NT)
            total = term if total is None else total + term
        if first:
            out_ref[side] = total
            continue
        total = total + dot(refs[whole + side][...], columns(steps[-1]), NT)
        hidden = (total * jax.nn.sigmoid(total)).astype(BF16)
        out_ref[:, side * even : (side + 1) * even] = hidden[:, 0:even]
        at = 2 * even + side * edge
        out_ref[:, at : at + edge] = hidden[:, even:units]


def down_kernel(steps, size, first, tp_ref, *refs):
    if first:
        pieces, total_ref, ends_ref = refs[: len(steps)], None, None
        blocks = [[piece.at[part] for piece in pieces] for part in range(2)]
    else:
        total_ref, ends_ref = refs[2:4]
        blocks = [[refs[0]], [refs[1]]]
    w_ref, out_ref = refs[-2:]
    rows, both = blocks[0][0].shape
    units = both // 2
    edge = units % 128
    even = units - edge

    def term(block, step, side):
        owner = lax.rem(tp_ref[0] + size - step, size)
        at = 2 * even + side * edge
        mine = jnp.concatenate(
            [block[:, side * even : (side + 1) * even], block[:, at : at + edge]], axis=1
        )
        return dot(mine, w_ref[pl.ds(pl.multiple_of(owner * units, 64), units), :])

    if not first:
        tail = ends_ref[...].astype(BF16)
        for d in range(out_ref.shape[0]):
            out_ref[d, 2 * CAPACITY : 2 * CAPACITY + 8, :] = tail
    for side in range(2):
        for part in range(2):
            span = slice(part * rows, (part + 1) * rows)
            total = None if first else total_ref[side, span]
            for step, block in zip(steps, blocks[part]):
                value = term(block, step, side)
                total = value if total is None else total + value
            if first:
                out_ref[side, span] = total
                continue
            total = total.astype(BF16)
            lanes = total.shape[1] // 2
            group = rows // CAPACITY
            for j in range(group):
                d = (side * 2 + part) * group + j
                mine = total[j * CAPACITY : (j + 1) * CAPACITY]
                out_ref[d, 0:CAPACITY, :] = mine[:, 0:lanes]
                out_ref[d, CAPACITY : 2 * CAPACITY, :] = mine[:, lanes:]


def stage(body, name, steps, pieces, rest, at, out):
    size = lax.axis_size("tp")
    operands = [*pieces, *rest]
    kernel = functools.partial(body, steps, size, len(rest) == 1)
    macs = len(steps) * pieces[0].size * rest[-1].size // pieces[0].shape[-1] // size
    moved = sum(v.size * v.dtype.itemsize for v in operands)
    return pl.pallas_call(
        kernel,
        out_shape=out,
        in_specs=[smem()] + [vmem()] * len(operands),
        out_specs=vmem(),
        cost_estimate=cost(2 * macs, moved),
        compiler_params=grant(20),
        name=name,
    )(at, *operands)


def up(block, w, at):
    _, half, _ = block.shape
    units = w.shape[0]
    middle = jax.ShapeDtypeStruct((2, half, units), F32)
    out = jax.ShapeDtypeStruct((half, 2 * units), BF16)
    pieces, far = ring(block, {})
    steps = steps_of(lax.axis_size("tp"))
    cut = len(pieces)
    total = stage(up_kernel, "up_near", steps[:cut], pieces[:cut], [w], at, middle)
    return stage(up_kernel, "up_far", steps[cut:], pieces[cut:] + far, [total, w], at, out)


def down(block, w, at, holds, ends):
    _, rows, _ = block.shape
    width = w.shape[1]
    middle = jax.ShapeDtypeStruct((2, 2 * rows, width), F32)
    out = jax.ShapeDtypeStruct((4 * rows // CAPACITY, 2 * CAPACITY + 8, width // 2), BF16)
    pieces, far = ring(block, holds)
    steps = steps_of(lax.axis_size("tp"))
    total = stage(down_kernel, "down_near", steps[:-1], pieces, [w], at, middle)
    return stage(down_kernel, "down_far", steps[-1:], far, [total, ends(), w], at, out)


def one_minus_exp(y):
    small = -y * (1.0 + y * (0.5 + y * (1.0 / 6 + y * (1.0 / 24 + y * (1.0 / 120 + y / 720)))))
    return jnp.where(y > -0.25, small, 1.0 - jnp.exp(y))


def local_kernel(x_ref, prev_ref, tap_ref, carry_ref, entry_ref, lane_ref, jump_ref, decay_ref, state_ref, ends_ref, pad_ref):
    channels, length = x_ref.shape
    pad_ref[0:8, :] = dot(same((8, length), length - 8).astype(BF16), prev_ref[...], NT)
    pad_ref[8 : 8 + length, :] = dot(same((length, length)).astype(BF16), x_ref[...], NT)
    taps = tap_ref[...].astype(F32)
    conv = jnp.zeros((length, channels), F32)
    for j in range(CONV):
        at = 8 - (CONV - 1) + j
        conv = conv + pad_ref[at : at + length, :] * taps[j : j + 1]
    half = conv.astype(BF16)
    recur = jax.nn.sigmoid(dot(half, carry_ref[0]))
    entry = jax.nn.sigmoid(dot(half, entry_ref[0]))
    fade = jnp.exp(-lane_ref[...])
    series = fade * (1.0 - fade * (0.5 - fade * (1.0 / 3 - fade * (0.25 - fade * 0.2))))
    soft = jnp.where(fade < 0.03, series, jnp.log(1.0 + fade))
    jump = jnp.sum(same((length, length)) * jump_ref[...], axis=1, keepdims=True)
    log_decay = -8.0 * recur * soft + jump
    state = jnp.sqrt(one_minus_exp(2.0 * log_decay)) * entry * conv
    decay = jnp.exp(log_decay)
    rows = lax.broadcasted_iota(jnp.int32, (length, channels), 0)
    step = 1
    while step < length:
        ready = rows >= step
        before_state = jnp.where(ready, pltpu.roll(state, step, 0), 0.0)
        before_decay = jnp.where(ready, pltpu.roll(decay, step, 0), 1.0)
        state = decay * before_state + state
        decay = decay * before_decay
        step *= 2
    decay_ref[...] = decay
    state_ref[...] = state
    ends_ref[...] = jnp.zeros((8, 128), F32)
    for k, value in enumerate((decay[length - 1 : length], state[length - 1 : length])):
        high = value.astype(BF16).astype(F32)
        for j, term in enumerate((high, value - high)):
            r = 2 * k + j
            ends_ref[r : r + 1, :] = term[:, 0:128]
            ends_ref[r + 4 : r + 5, 0 : channels - 128] = term[:, 128:channels]


def local_scan(x, prev, taps, carry, entry, lane, jump):
    channels, length = x.shape
    full = jax.ShapeDtypeStruct((length, channels), F32)
    return pl.pallas_call(
        local_kernel,
        out_shape=(full, full, jax.ShapeDtypeStruct((8, 128), F32)),
        in_specs=[vmem()] * 7,
        out_specs=(vmem(), vmem(), vmem()),
        scratch_shapes=[pltpu.VMEM((length + 8, channels), F32)],
        cost_estimate=cost(100 * length * channels, 16 * length * channels),
        compiler_params=grant(6),
        name="local_scan",
    )(x, prev, taps, carry, entry, lane, jump)


def here(axis):
    return lax.axis_index(axis).astype(jnp.int32).reshape(1)


def on_device(x, valve, taps, carry, entry, lane, jump, tok, scale, routes, scores, expand, contract):
    ep = lax.axis_size("ep")
    width = tok.shape[1] // lax.axis_size("tp")
    at = here("tp")
    sent = dispatch(tok, scale[None, :], routes.T, at, ep, width)
    arrived = lax.all_to_all(sent.reshape(ep, CAPACITY, width), "ep", 0, 0, tiled=True)
    half = ep * CAPACITY // 2
    hidden = up(arrived.reshape(2, half, width), expand[0].T, at)
    hidden, flipped = lax.optimization_barrier((hidden, x.T))
    prev = lax.ppermute(flipped, "ep", [(i, i + 1) for i in range(ep - 1)])
    kept = {}

    def hold_prev(block):
        block, kept["prev"] = lax.optimization_barrier((block, prev))
        return block

    def hold_scan(block):
        local = local_scan(flipped, kept["prev"], taps, carry, entry, lane[None, :], jump[None, :])
        block, kept["local"] = lax.optimization_barrier((block, local))
        return block

    holds = {1: hold_prev, 2: hold_scan}
    blocks = hidden.reshape(2, half // 2, -1)
    done = down(blocks, contract[0], at, holds, lambda: kept["local"][2])
    decay, state, _ = kept["local"]
    returned = lax.all_to_all(done, "ep", 0, 0, tiled=True)
    moe, mixed = finish(returned, routes, scores, decay, state, valve.T, here("ep"))
    return (mixed.T, moe)


def solution(mesh):
    rows = P(("grp", "ep"), None)
    split = P(("grp", "ep"), "tp")
    placed = (
        split,
        split,
        P(None, "tp"),
        P("tp", None, None),
        P("tp", None, None),
        P("tp"),
        P(("grp", "ep")),
        rows,
        P(),
        rows,
        rows,
        P("ep", None, "tp"),
        P("ep", None, "tp"),
    )
    return jax.shard_map(
        on_device, mesh=mesh, in_specs=placed, out_specs=(split, split), check_vma=False
    )
```
